128 devices in a mesh: sp: 16 (over z, x), fs: 4 (over y), tp: 2 (over core).
Axes of the slice: x: 4, y: 4, z: 4, core: 2. Of those that a mesh axis runs over, the one named last changes fastest.
Arguments:
- tokens: bfloat16 [4, 16384, 2048], P('fs', ('sp', 'tp')), may hold values from -6 to 6
- norm_gain: bfloat16 [2048], replicated, may hold values from 0.099609375 to 1.8984375
- w_query: bfloat16 [2048, 1024], P(None, 'tp'), may hold values from -0.125 to 0.125
- w_key: bfloat16 [2048, 1024], P(None, 'tp'), may hold values from -0.125 to 0.125
- w_value: bfloat16 [2048, 1024], P(None, 'tp'), may hold values from -0.125 to 0.125
- w_outgate: bfloat16 [2048, 1024], P(None, 'tp'), may hold values from -0.125 to 0.125
- w_gatein: bfloat16 [2048, 1024], P(None, 'tp'), may hold values from -0.125 to 0.125
- w_gateout: bfloat16 [2048, 1024], P(None, 'tp'), may hold values from -0.125 to 0.125
- w_convin: bfloat16 [2048, 1024], P(None, 'tp'), may hold values from -0.125 to 0.125
- w_igate: bfloat16 [2048, 8], replicated, may hold values from -0.125 to 0.125
- w_fgate: bfloat16 [2048, 8], replicated, may hold values from -0.125 to 0.125
- input_bias: float32 [8], replicated, may hold values from -1 to 101
- forget_bias: float32 [8], replicated
- forget_extra: float32 [4, 16384, 8], P('fs', 'sp', 'tp'), may hold values from -0.7 to 0
- init_memory: float32 [4, 8, 128, 128], P('fs', 'tp'), may hold values from -112 to 112
- head_gain: bfloat16 [1024], replicated, may hold values from 0.099609375 to 1.8984375
- conv_taps: bfloat16 [3, 1024], replicated, may hold values from -3.5 to 3.5
- out_memory: bfloat16 [1024, 2048], P('tp'), may hold values from -0.125 to 0.125
- out_conv: bfloat16 [1024, 2048], P('tp'), may hold values from -0.125 to 0.125
Outputs:
- layer_out: bfloat16 [4, 16384, 2048], P('fs', ('sp', 'tp'))
The draws below stay inside these ranges and needn't reach their ends.
All inputs are finite; a program needn't handle non-finite values.
Results may differ from the reference program's by a relative error of at most 0.017.
Values may be sent and summed in bfloat16 or wider, within the bound.
A program may use at most 128 MiB of HBM per device.

```python
import math
import jax
import jax.numpy as jnp
from jax import lax

D = 2048
MEMORY_HEADS = 8
DH = 128
HALF = 1024
BLOCK = 128
TAPS = 3
TOK_DEV = 1024
SEQUENCE_COUNT = 4
SEQUENCE_LENGTH = 16384
N_TP = 2


def draw_input_bias(key, part):
    base_key = jax.random.fold_in(jax.random.fold_in(key, 11), 0)
    steady_forget = jax.random.uniform(base_key, (MEMORY_HEADS,), jnp.float32, -1.0, 1.0)
    return steady_forget


def draw_forget_bias(key, part):
    slow_key, fast_key, pick_key = jax.random.split(jax.random.fold_in(key, 23), 3)
    slow_bias = math.log(SEQUENCE_LENGTH) + jax.random.uniform(slow_key, (MEMORY_HEADS,), jnp.float32, 1.5, 3.0)
    fast_bias = jax.random.uniform(fast_key, (MEMORY_HEADS,), jnp.float32, 3.4, 4.6)
    chosen = jax.random.permutation(pick_key, MEMORY_HEADS) < MEMORY_HEADS // 2
    return jnp.where(chosen, fast_bias, slow_bias)


def draw_forget_extra(key, part):
    rate_key, place_random_key, drop_random_key = jax.random.split(jax.random.fold_in(key, 37), 3)
    span_count = SEQUENCE_LENGTH // TOK_DEV
    span_rates = jnp.exp(jax.random.uniform(rate_key, (SEQUENCE_COUNT, span_count, 1, MEMORY_HEADS), jnp.float32, math.log(0.1), math.log(0.8))) / SEQUENCE_LENGTH
    steady_forget = -jnp.broadcast_to(span_rates, (SEQUENCE_COUNT, span_count, TOK_DEV, MEMORY_HEADS)).reshape(SEQUENCE_COUNT, SEQUENCE_LENGTH, MEMORY_HEADS)
    sudden_drop_places = jax.random.randint(place_random_key, (SEQUENCE_COUNT, 2), 0, SEQUENCE_LENGTH)
    sudden_drop_mask = jnp.any(jnp.arange(SEQUENCE_LENGTH)[None, :, None] == sudden_drop_places[:, None, :], axis=-1)
    sudden_drop_values = jax.random.uniform(drop_random_key, (SEQUENCE_COUNT, SEQUENCE_LENGTH, MEMORY_HEADS), jnp.float32, math.log(0.5), math.log(0.8))
    return steady_forget + jnp.where(sudden_drop_mask[:, :, None], sudden_drop_values, 0.0)


def shard_levels(key, extent, cuts, smallest, top_value):
    level = 1.0
    for dim, parts in cuts:
        steps = jax.random.uniform(jax.random.fold_in(jax.random.fold_in(key, 6), dim), (parts,), jnp.float32, smallest / len(cuts), top_value / len(cuts))
        level = level * jnp.repeat(jnp.exp(steps), extent[dim] // parts).reshape((-1,) + (1,) * (len(extent) - 1 - dim))
    return level


def gaussian(own_key, extent, spread, reach, shards=(), held_as=jnp.bfloat16):
    result = spread * jax.random.normal(own_key, extent, jnp.float32)
    if shards:
        result = result * shard_levels(own_key, extent, shards, -0.22, 0.18)
    return jnp.clip(result, -reach, reach).astype(held_as)


def setup_inputs(seed: int = 0) -> dict:
    seeds = jax.random.split(jax.random.key(seed), 20)
    return {
        "tokens": gaussian(seeds[0], (SEQUENCE_COUNT, SEQUENCE_LENGTH, D), 1.0, 6.0, ((0, 4), (1, 32))),
        "norm_gain": jnp.clip(1.0 + 0.18 * jax.random.normal(seeds[1], (D,), jnp.float32), 0.099609375, 1.8984375).astype(jnp.bfloat16),
        "w_query": gaussian(seeds[2], (D, HALF), D ** -0.5, 0.125, ((1, 2),)),
        "w_key": gaussian(seeds[3], (D, HALF), D ** -0.5, 0.125, ((1, 2),)),
        "w_value": gaussian(seeds[4], (D, HALF), D ** -0.5, 0.125, ((1, 2),)),
        "w_outgate": gaussian(seeds[5], (D, HALF), D ** -0.5, 0.125, ((1, 2),)),
        "w_gatein": gaussian(seeds[6], (D, HALF), D ** -0.5, 0.125, ((1, 2),)),
        "w_gateout": gaussian(seeds[7], (D, HALF), D ** -0.5, 0.125, ((1, 2),)),
        "w_convin": gaussian(seeds[8], (D, HALF), D ** -0.5, 0.125, ((1, 2),)),
        "w_igate": gaussian(seeds[9], (D, MEMORY_HEADS), D ** -0.5, 0.125),
        "w_fgate": gaussian(seeds[10], (D, MEMORY_HEADS), D ** -0.5, 0.125),
        "input_bias": draw_input_bias(jax.random.fold_in(seeds[19], 71), 0),
        "forget_bias": draw_forget_bias(jax.random.fold_in(seeds[19], 71), 0),
        "forget_extra": draw_forget_extra(jax.random.fold_in(seeds[19], 71), 0),
        "init_memory": gaussian(seeds[14], (SEQUENCE_COUNT, MEMORY_HEADS, DH, DH), (0.15 * SEQUENCE_LENGTH ** 0.5), 112.0, ((0, 4), (1, 2)), jnp.float32),
        "head_gain": jnp.clip(1.0 + 0.18 * jax.random.normal(seeds[15], (HALF,), jnp.float32), 0.099609375, 1.8984375).astype(jnp.bfloat16),
        "conv_taps": gaussian(seeds[16], (TAPS, HALF), TAPS ** -0.5, 3.5),
        "out_memory": gaussian(seeds[17], (HALF, D), (2 * HALF) ** -0.5, 0.125, ((0, 2),)),
        "out_conv": gaussian(seeds[18], (HALF, D), (2 * HALF) ** -0.5, 0.125, ((0, 2),)),
    }


EPSILON = 1e-06

def memory_cell(queries, key_rows, value_rows, input_pre, log_forget, start_memory):
    nblocks = SEQUENCE_LENGTH // BLOCK
    key_factor = DH ** (-0.5)
    highest = lax.Precision.HIGHEST

    def blocked(matrix):
        return jnp.swapaxes(matrix.reshape(nblocks, BLOCK, MEMORY_HEADS, DH), 1, 2).astype(jnp.float32)

    def gate_blocks(matrix):
        return jnp.swapaxes(matrix.reshape(nblocks, BLOCK, MEMORY_HEADS), 1, 2)
    causal = jnp.tril(jnp.ones((BLOCK, BLOCK), dtype=bool))

    def advance(memory_pair, inputs):
        memory, log_scale = memory_pair
        query_blk, key_blk, value_blk, gate_in_blk, forget_blk = inputs
        cumulative = jnp.cumsum(forget_blk, axis=-1)
        block_total = cumulative[:, -1]
        exponent = block_total[:, None] - cumulative + gate_in_blk
        block_top = lax.optimization_barrier(jnp.max(exponent, axis=-1))
        weighted_keys = (jnp.exp(exponent - block_top[:, None])[:, :, None] * key_blk * key_factor).astype(jnp.bfloat16)
        weighted_keys = lax.optimization_barrier(weighted_keys).astype(jnp.float32)
        block_terms = jnp.einsum('hsd,hse->hde', weighted_keys, value_blk, precision=highest)
        pair_log = cumulative[:, :, None] - cumulative[:, None, :] + gate_in_blk[:, None, :]
        pair_log = jnp.where(causal, pair_log, -jnp.inf)
        carried_log = cumulative + log_scale[:, None]
        row_top = jnp.maximum(carried_log, lax.optimization_barrier(jnp.max(pair_log, axis=-1)))
        scores = jnp.einsum('htd,hsd->hts', query_blk, key_blk, precision=highest) * key_factor
        weighted = (jnp.exp(pair_log - row_top[:, :, None]) * scores).astype(jnp.bfloat16)
        weighted = lax.optimization_barrier(weighted).astype(jnp.float32)
        carried = jnp.einsum('htd,hde->hte', query_blk, memory, precision=highest)
        readout = jnp.exp(carried_log - row_top)[:, :, None] * carried
        readout = readout + jnp.einsum('hts,hse->hte', weighted, value_blk, precision=highest)
        new_scale = jnp.maximum(block_total + log_scale, block_top)
        new_memory = jnp.exp(block_total + log_scale - new_scale)[:, None, None] * memory
        new_memory = new_memory + jnp.exp(block_top - new_scale)[:, None, None] * block_terms
        return ((new_memory, new_scale), readout)
    start_pair = (start_memory, jnp.zeros((MEMORY_HEADS,), jnp.float32))
    inputs = (blocked(queries), blocked(key_rows), blocked(value_rows), gate_blocks(input_pre), gate_blocks(log_forget))
    final_pair, readouts = lax.scan(advance, start_pair, inputs)
    return jnp.swapaxes(readouts, 1, 2).reshape(SEQUENCE_LENGTH, HALF)

def reference(tokens, norm_gain, w_query, w_key, w_value, w_outgate, w_gatein, w_gateout, w_convin, w_igate, w_fgate, input_bias, forget_bias, forget_extra, init_memory, head_gain, conv_taps, out_memory, out_conv):
    group_width = HALF // N_TP
    outputs = []
    for seq_index in range(SEQUENCE_COUNT):
        seq_rows = tokens[seq_index].astype(jnp.float32)
        normed = seq_rows * lax.rsqrt(lax.optimization_barrier(jnp.mean(seq_rows * seq_rows, axis=-1, keepdims=True)) + EPSILON)
        normed = (normed * norm_gain.astype(jnp.float32)).astype(jnp.bfloat16)

        def project(weight):
            return jnp.dot(normed, weight, preferred_element_type=jnp.float32).astype(jnp.bfloat16)
        queries = project(w_query)
        key_rows = project(w_key)
        value_rows = project(w_value)
        out_gate = project(w_outgate)
        gate_in = project(w_gatein)
        gate_out = project(w_gateout)
        conv_input = project(w_convin)
        input_pre = jnp.dot(normed, w_igate, preferred_element_type=jnp.float32) + input_bias
        forget_pre = jnp.dot(normed, w_fgate, preferred_element_type=jnp.float32) + forget_bias
        log_forget = jax.nn.log_sigmoid(forget_pre) + forget_extra[seq_index]
        readout = memory_cell(queries, key_rows, value_rows, input_pre, log_forget, init_memory[seq_index])
        per_head = readout.reshape(SEQUENCE_LENGTH, MEMORY_HEADS, DH)
        normalized = per_head * lax.rsqrt(lax.optimization_barrier(jnp.mean(per_head * per_head, axis=-1, keepdims=True)) + EPSILON)
        memory_out = normalized.reshape(SEQUENCE_LENGTH, HALF) * head_gain.astype(jnp.float32) * jax.nn.sigmoid(out_gate.astype(jnp.float32))
        memory_out = memory_out.astype(jnp.bfloat16)
        conv_product = (gate_in.astype(jnp.float32) * conv_input.astype(jnp.float32)).astype(jnp.bfloat16)
        conv_product = lax.optimization_barrier(conv_product).astype(jnp.float32)
        padded = jnp.pad(conv_product, ((TAPS - 1, 0), (0, 0)))
        mixed_conv = jnp.zeros((SEQUENCE_LENGTH, HALF), jnp.float32)
        for tap_index in range(TAPS):
            mixed_conv = mixed_conv + padded[tap_index:tap_index + SEQUENCE_LENGTH] * conv_taps[tap_index].astype(jnp.float32)
        conv_out = (gate_out.astype(jnp.float32) * mixed_conv).astype(jnp.bfloat16)
        summed = jnp.zeros((SEQUENCE_LENGTH, D), jnp.float32)
        for part_index in range(N_TP):
            low_col = part_index * group_width
            high_col = low_col + group_width
            partial_value = jnp.dot(memory_out[:, low_col:high_col], out_memory[low_col:high_col], preferred_element_type=jnp.float32)
            partial_value = partial_value + jnp.dot(conv_out[:, low_col:high_col], out_conv[low_col:high_col], preferred_element_type=jnp.float32)
            summed = summed + lax.optimization_barrier(partial_value.astype(jnp.bfloat16)).astype(jnp.float32)
        outputs.append(summed.astype(jnp.bfloat16))
    return jnp.stack(outputs)
```

```python
import functools
import math

import jax
import jax.numpy as jnp
from jax import lax
from jax.experimental import pallas as pl
from jax.experimental.pallas import tpu as pltpu
from jax.sharding import PartitionSpec as P

MESH = pl.DeviceIdType.MESH
F32 = jnp.float32
BF16 = jnp.bfloat16
BLOCK = 128
EPSILON = 1e-06
LOWEST_LOG = -1e30

K_, V_, Q_, OG_, GI_, CI_, GO_ = range(7)
T_BIAS, T_KW, T_ALPHA, T_BETA, T_TOP, T_CARRY = range(6)
L_TOK, L_WIG, L_WFG, L_GAIN, L_FE, L_IB, L_FB, L_TAPS, L_HG, L_OM, L_OC, L_INIT, L_OUT, L_W = (
    0, 1, 2, 3, 4, 5, 6, 7, 8, 9, 10, 11, 12, 16,
)


def kernel(
    n_sp,
    tokens, norm_gain, w_query, w_key, w_value, w_outgate, w_gatein, w_gateout, w_convin,
    w_igate, w_fgate, input_bias, forget_bias, forget_extra, init_memory, head_gain, conv_taps,
    out_memory, out_conv,
    out,
    tok, gain, x, w, wo, wig, wfg, wg, proj, gates, fe, ib, fb, taps, hg, init,
    keys_t, prefix, table, cols, mix, seg, seg_in, scal, scal_in, state_out, state_in,
    rim_in, read, sig, conv, both, part, part_in,
    lsem, tok_s, tok_r, seg_s, seg_r, scal_s, scal_r, st_s, st_r, rim_s, rim_r, out_s, out_r,
):
    own = tokens.shape[1]
    width = tokens.shape[2]
    count = 2 * own
    local_width = w_query.shape[1]
    heads = init_memory.shape[1]
    dh = init_memory.shape[3]
    nblocks = count // BLOCK
    slice_rows = heads * dh // n_sp
    key_log = -0.5 * math.log(dh)
    me = lax.axis_index("sp")
    side = lax.axis_index("tp")
    other = 1 - side
    my_row = pl.multiple_of(side * own, own)
    peer_row = pl.multiple_of(other * own, own)
    my_head = (me * slice_rows) // dh
    my_depth = pl.multiple_of(me * slice_rows - my_head * dh, slice_rows)
    my_lane = pl.multiple_of(side * local_width, local_width)

    def local(src, dst, index):
        return pltpu.make_async_copy(src, dst, lsem.at[index])

    weights = (w_key, w_value, w_query, w_outgate, w_gatein, w_convin, w_gateout)

    barrier = pltpu.get_barrier_semaphore()
    pl.semaphore_signal(barrier, inc=1, device_id={"tp": other}, device_id_type=MESH)

    def greet(k, carry):
        pl.semaphore_signal(
            barrier, inc=1, device_id={"sp": lax.rem(me + k, n_sp)}, device_id_type=MESH
        )
        return carry

    lax.fori_loop(1, n_sp, greet, 0)

    first = [
        local(tokens.at[0], tok, L_TOK),
        local(norm_gain, gain, L_GAIN),
        local(w_igate, wig, L_WIG),
        local(w_fgate, wfg, L_WFG),
        local(w_key, w.at[K_], L_W + K_),
        local(w_value, w.at[V_], L_W + V_),
    ]
    later = [
        local(weights[p], w.at[p], L_W + p) for p in range(2, 7)
    ] + [
        local(forget_extra.at[0], fe, L_FE),
        local(input_bias, ib, L_IB),
        local(forget_bias, fb, L_FB),
        local(conv_taps, taps, L_TAPS),
        local(head_gain, hg, L_HG),
        local(init_memory.at[0, my_head, pl.ds(my_depth, slice_rows), :], init, L_INIT),
        local(out_memory, wo.at[pl.ds(0, local_width), :], L_OM),
        local(out_conv, wo.at[pl.ds(local_width, local_width), :], L_OC),
    ]
    for copy in first:
        copy.start()
    first[1].wait()
    first[0].wait()
    for copy in later:
        copy.start()

    gain_row = gain[...].astype(F32)
    step_rows = 64

    def norm_step(i, carry):
        rows = pl.multiple_of(i * step_rows, step_rows)
        values = tok[pl.ds(rows, step_rows), :].astype(F32)
        scale = lax.rsqrt(jnp.mean(values * values, axis=-1, keepdims=True) + EPSILON)
        x[pl.ds(my_row + rows, step_rows), :] = (values * scale * gain_row).astype(BF16)
        return carry

    lax.fori_loop(0, own // step_rows, norm_step, 0)

    first[2].wait()
    first[3].wait()
    narrow = wig.shape[1]
    wg[:, 0:narrow] = wig[...]
    wg[:, narrow : 2 * narrow] = wfg[...]
    wg[:, 2 * narrow :] = jnp.zeros((width, wg.shape[1] - 2 * narrow), BF16)

    def gate_dot(row):
        gates[pl.ds(row, own), :] = jnp.dot(
            x[pl.ds(row, own), :], wg[...], preferred_element_type=F32
        )

    def project(row, start, stop, wait):
        def step(p, carry):
            if wait:
                pltpu.make_async_copy(w_query, w.at[p], lsem.at[L_W + p]).wait()
            proj[p, pl.ds(row, own), :] = jnp.dot(
                x[pl.ds(row, own), :], w[p], preferred_element_type=F32
            ).astype(BF16)
            return carry

        lax.fori_loop(start, stop, step, 0)

    project(my_row, 0, 2, True)
    gate_dot(my_row)

    pl.semaphore_wait(barrier, n_sp)
    send_rows = pltpu.make_async_remote_copy(
        src_ref=x.at[pl.ds(my_row, own), :],
        dst_ref=x.at[pl.ds(my_row, own), :],
        send_sem=tok_s, recv_sem=tok_r,
        device_id={"tp": other}, device_id_type=MESH,
    )
    send_rows.start()
    project(my_row, 2, 7, True)
    take_rows = pltpu.make_async_remote_copy(
        src_ref=x.at[pl.ds(peer_row, own), :],
        dst_ref=x.at[pl.ds(peer_row, own), :],
        send_sem=tok_s, recv_sem=tok_r,
        device_id={"tp": other}, device_id_type=MESH,
    )
    take_rows.wait_recv()
    project(peer_row, 0, 2, False)
    gate_dot(peer_row)

    for copy in later[5:8]:
        copy.wait()
    lanes = lax.broadcasted_iota(jnp.int32, (nblocks * heads, BLOCK), 1)
    head_rows = lax.broadcasted_iota(jnp.int32, (heads, BLOCK), 0)
    bias_in = jnp.zeros((heads, BLOCK), F32)
    bias_forget = jnp.zeros((heads, BLOCK), F32)
    for h in range(heads):
        for part_index in range(2):
            pick = (head_rows == h) & (side == part_index)
            c = part_index * heads + h
            bias_in = jnp.where(pick, ib[0:1, c : c + 1], bias_in)
            bias_forget = jnp.where(pick, fb[0:1, c : c + 1], bias_forget)
    ins, forgets = [], []
    pad = jnp.zeros((BLOCK, BLOCK - heads), F32)
    for b in range(nblocks):
        turned = gates[b * BLOCK : (b + 1) * BLOCK, :].T
        extra = jnp.concatenate([fe[b * BLOCK : (b + 1) * BLOCK, :], pad], axis=1).T
        pre_in = jnp.where(side == 0, turned[0:heads], turned[heads : 2 * heads])
        pre_forget = jnp.where(
            side == 0, turned[2 * heads : 3 * heads], turned[3 * heads : 4 * heads]
        )
        ins.append(pre_in + bias_in)
        forget = pre_forget + bias_forget
        forgets.append(
            jnp.minimum(forget, 0.0) - jnp.log1p(jnp.exp(-jnp.abs(forget))) + extra[0:heads]
        )
    ins = jnp.concatenate(ins, axis=0)
    cumulative = jnp.concatenate(forgets, axis=0)
    shift = 1
    while shift < BLOCK:
        cumulative = cumulative + jnp.where(
            lanes >= shift, pltpu.roll(cumulative, shift, 1), 0.0
        )
        shift *= 2
    pair = ins - cumulative
    top = pair
    shift = 1
    while shift < BLOCK:
        top = jnp.maximum(top, jnp.where(lanes >= shift, pltpu.roll(top, shift, 1), top))
        shift *= 2
    total = jnp.broadcast_to(cumulative[:, BLOCK - 1 :], cumulative.shape)
    last_top = jnp.broadcast_to(top[:, BLOCK - 1 :], top.shape)
    log_scale = jnp.full((heads, BLOCK), LOWEST_LOG, F32)
    before = jnp.zeros((heads, BLOCK), F32)
    scales, befores, alphas, betas = [], [], [], []
    for b in range(nblocks):
        block_total = total[b * heads : (b + 1) * heads]
        block_top = block_total + last_top[b * heads : (b + 1) * heads]
        scales.append(log_scale)
        befores.append(before)
        merged = jnp.maximum(block_total + log_scale, block_top)
        alphas.append(jnp.exp(block_total + log_scale - merged))
        betas.append(jnp.exp(block_top - merged))
        log_scale = merged
        before = before + block_total
    scal[0:heads, :] = before
    scal[heads : 2 * heads, :] = log_scale
    scales = jnp.concatenate(scales, axis=0)
    row_top = jnp.maximum(scales, top)
    table[T_BIAS] = pair + key_log
    table[T_KW] = jnp.exp(pair + key_log - last_top)
    table[T_ALPHA] = jnp.concatenate(alphas, axis=0)
    table[T_BETA] = jnp.concatenate(betas, axis=0)
    table[T_TOP] = row_top
    table[T_CARRY] = jnp.concatenate(befores, axis=0)
    carry_weight = jnp.exp(scales - row_top)
    fill = jnp.zeros((BLOCK - 2 * heads, BLOCK), F32)
    for b in range(nblocks):
        rows = slice(b * heads, (b + 1) * heads)
        cols[b] = jnp.concatenate([row_top[rows], carry_weight[rows], fill], axis=0).T

    scal_in[me] = scal[...]

    def send_scales(k, carry):
        target = lax.rem(me + k, n_sp)
        pltpu.make_async_remote_copy(
            src_ref=scal, dst_ref=scal_in.at[me],
            send_sem=scal_s.at[target], recv_sem=scal_r.at[me],
            device_id={"sp": target}, device_id_type=MESH,
        ).start()
        return carry

    lax.fori_loop(1, n_sp, send_scales, 0)

    for h in range(heads):
        mix[h] = jnp.zeros((dh, dh), F32)

    def terms_step(b, carry):
        rows = pl.ds(pl.multiple_of(b * BLOCK, BLOCK), BLOCK)
        for h in range(heads):
            at = pl.ds(b * heads + h, 1)
            hs = slice(h * dh, (h + 1) * dh)
            turned = proj[K_, rows, hs].T
            keys_t[b, h] = turned
            weighted = (turned.astype(F32) * table[T_KW, at, :]).astype(BF16)
            terms = jnp.dot(weighted, proj[V_, rows, hs], preferred_element_type=F32)
            held = mix[h]
            prefix[b, h] = held.astype(BF16)
            mix[h] = table[T_ALPHA, at, :] * held + table[T_BETA, at, :] * terms
        return carry

    lax.fori_loop(0, nblocks, terms_step, 0)
    for h in range(heads):
        per_head = dh // slice_rows
        for piece in range(per_head):
            seg[h * per_head + piece] = mix[
                h, piece * slice_rows : (piece + 1) * slice_rows, :
            ].astype(BF16)
    seg_in[me] = seg[me]

    def send_segment(k, carry):
        target = lax.rem(me + k, n_sp)
        pltpu.make_async_remote_copy(
            src_ref=seg.at[target], dst_ref=seg_in.at[me],
            send_sem=seg_s.at[target], recv_sem=seg_r.at[me],
            device_id={"sp": target}, device_id_type=MESH,
        ).start()
        return carry

    lax.fori_loop(1, n_sp, send_segment, 0)

    project(peer_row, GI_, GO_, False)
    conv_rows = 64

    def product_step(i, carry):
        rows = pl.multiple_of(i * conv_rows, conv_rows)
        conv[pl.ds(rows + 8, conv_rows), :] = (
            (
                proj[GI_, pl.ds(rows, conv_rows), :].astype(F32)
                * proj[CI_, pl.ds(rows, conv_rows), :].astype(F32)
            )
            .astype(BF16)
            .astype(F32)
        )
        return carry

    lax.fori_loop(0, count // conv_rows, product_step, 0)
    following = lax.rem(me + 1, n_sp)
    rim = pltpu.make_async_remote_copy(
        src_ref=conv.at[pl.ds(count, 8), :], dst_ref=rim_in,
        send_sem=rim_s, recv_sem=rim_r,
        device_id={"sp": following}, device_id_type=MESH,
    )
    rim.start()
    project(peer_row, Q_, GI_, False)

    def wait_from(src, dst, send, recv):
        def step(k, carry):
            source = lax.rem(me + k, n_sp)
            pltpu.make_async_remote_copy(
                src_ref=src.at[source] if src is not scal else src,
                dst_ref=dst.at[source],
                send_sem=send.at[source], recv_sem=recv.at[source],
                device_id={"sp": source}, device_id_type=MESH,
            ).wait_recv()
            return carry

        lax.fori_loop(1, n_sp, step, 0)

    wait_from(scal, scal_in, scal_s, scal_r)
    wait_from(seg, seg_in, seg_s, seg_r)
    later[10].wait()
    state = init[...]
    state_log = jnp.zeros((1, BLOCK), F32)
    for i in range(n_sp):
        state_out[i] = state.astype(BF16)
        if i == n_sp - 1:
            break
        span = scal_in[i, pl.ds(my_head, 1), :]
        span_top = scal_in[i, pl.ds(heads + my_head, 1), :]
        merged = jnp.maximum(span + state_log, span_top)
        state = (
            jnp.exp(span + state_log - merged) * state
            + jnp.exp(span_top - merged) * seg_in[i].astype(F32)
        )
        state_log = merged
    state_in[me] = state_out[me]

    def send_state(k, carry):
        target = lax.rem(me + k, n_sp)
        pltpu.make_async_remote_copy(
            src_ref=state_out.at[target], dst_ref=state_in.at[me],
            send_sem=st_s.at[target], recv_sem=st_r.at[me],
            device_id={"sp": target}, device_id_type=MESH,
        ).start()
        return carry

    lax.fori_loop(1, n_sp, send_state, 0)
    project(peer_row, GO_, GO_ + 1, False)

    start_log = jnp.zeros((heads, BLOCK), F32)
    for i in range(n_sp - 1):
        merged = jnp.maximum(scal_in[i, 0:heads, :] + start_log, scal_in[i, heads : 2 * heads, :])
        start_log = jnp.where(i < me, merged, start_log)

    t_index = lax.broadcasted_iota(jnp.int32, (BLOCK, BLOCK), 0)
    s_index = lax.broadcasted_iota(jnp.int32, (BLOCK, BLOCK), 1)
    causal = s_index <= t_index
    later[9].wait()
    later[8].wait()
    head_row = hg[:, pl.ds(my_lane, local_width)].astype(F32)

    def read_step(b, carry):
        rows = pl.ds(pl.multiple_of(b * BLOCK, BLOCK), BLOCK)
        columns = cols[b]
        for h in range(heads):
            at = pl.ds(b * heads + h, 1)
            hs = slice(h * dh, (h + 1) * dh)
            query = proj[Q_, rows, hs]
            scores = jnp.dot(query, keys_t[b, h], preferred_element_type=F32)
            log_weight = jnp.where(
                causal, table[T_BIAS, at, :] - columns[:, h : h + 1], -jnp.inf
            )
            weighted = (jnp.exp(log_weight) * scores).astype(BF16)
            read[rows, hs] = jnp.dot(
                weighted, proj[V_, rows, hs], preferred_element_type=F32
            ) + columns[:, heads + h : heads + h + 1] * jnp.dot(
                query, prefix[b, h], preferred_element_type=F32
            )
        sig[rows, :] = head_row * jax.nn.sigmoid(proj[OG_, rows, :].astype(F32))
        return carry

    lax.fori_loop(0, nblocks, read_step, 0)

    pltpu.make_async_remote_copy(
        src_ref=conv.at[pl.ds(count, 8), :], dst_ref=rim_in,
        send_sem=rim_s, recv_sem=rim_r,
        device_id={"sp": following}, device_id_type=MESH,
    ).wait_recv()
    conv[0:8, :] = jnp.where(me == 0, 0.0, rim_in[...])
    tap_rows = taps[:, pl.ds(my_lane, local_width)].astype(F32)

    def conv_step(i, carry):
        rows = pl.multiple_of(i * conv_rows, conv_rows)
        window = conv[pl.ds(rows, conv_rows + 8), :]
        mixed = window[6 : 6 + conv_rows] * tap_rows[0:1]
        mixed = mixed + window[7 : 7 + conv_rows] * tap_rows[1:2]
        mixed = mixed + window[8 : 8 + conv_rows] * tap_rows[2:3]
        both[pl.ds(rows, conv_rows), local_width:] = (
            proj[GO_, pl.ds(rows, conv_rows), :].astype(F32) * mixed
        ).astype(BF16)
        return carry

    lax.fori_loop(0, count // conv_rows, conv_step, 0)

    carried_log = table[T_CARRY] + jnp.concatenate([start_log] * nblocks, axis=0)
    new_top = jnp.maximum(table[T_TOP], carried_log)
    keep = jnp.exp(table[T_TOP] - new_top)
    bring = jnp.exp(carried_log - new_top)
    for b in range(nblocks):
        rows = slice(b * heads, (b + 1) * heads)
        cols[b] = jnp.concatenate([keep[rows], bring[rows], fill], axis=0).T
    wait_from(state_out, state_in, st_s, st_r)
    later[11].wait()
    later[12].wait()
    per_head = dh // slice_rows

    def finish_rows(row):
        def step(i, carry):
            b = row // BLOCK + i
            rows = pl.ds(pl.multiple_of(b * BLOCK, BLOCK), BLOCK)
            columns = cols[b]
            for h in range(heads):
                hs = slice(h * dh, (h + 1) * dh)
                start = state_in[h * per_head : (h + 1) * per_head].reshape(dh, dh)
                readout = columns[:, h : h + 1] * read[rows, hs] + columns[
                    :, heads + h : heads + h + 1
                ] * jnp.dot(proj[Q_, rows, hs], start, preferred_element_type=F32)
                normalized = readout * lax.rsqrt(
                    jnp.mean(readout * readout, axis=-1, keepdims=True) + EPSILON
                )
                both[rows, hs] = (normalized * sig[rows, hs]).astype(BF16)
            return carry

        lax.fori_loop(0, own // BLOCK, step, 0)

    finish_rows(peer_row)
    pieces = 2
    piece_rows = own // pieces

    def send_part(i):
        return pltpu.make_async_remote_copy(
            src_ref=part.at[pl.ds(i * piece_rows, piece_rows), :],
            dst_ref=part_in.at[pl.ds(i * piece_rows, piece_rows), :],
            send_sem=out_s.at[i], recv_sem=out_r.at[i],
            device_id={"tp": other}, device_id_type=MESH,
        )

    for i in range(pieces):
        part[pl.ds(i * piece_rows, piece_rows), :] = jnp.dot(
            both[pl.ds(peer_row + i * piece_rows, piece_rows), :], wo[...],
            preferred_element_type=F32,
        ).astype(BF16)
        send_part(i).start()
    finish_rows(my_row)
    stores = []
    for i in range(pieces):
        mine = jnp.dot(
            both[pl.ds(my_row + i * piece_rows, piece_rows), :], wo[...],
            preferred_element_type=F32,
        ).astype(BF16)
        rows = pl.ds(i * piece_rows, piece_rows)
        send_part(i).wait_recv()
        tok[rows, :] = (mine.astype(F32) + part_in[rows, :].astype(F32)).astype(BF16)
        store = local(tok.at[rows, :], out.at[0, rows, :], L_OUT + i)
        store.start()
        stores.append(store)

    send_rows.wait_send()
    rim.wait_send()

    def drain(k, carry):
        target = lax.rem(me + k, n_sp)
        for src, send, recv, dst in (
            (scal, scal_s, scal_r, scal_in.at[me]),
            (seg.at[target], seg_s, seg_r, seg_in.at[me]),
            (state_out.at[target], st_s, st_r, state_in.at[me]),
        ):
            pltpu.make_async_remote_copy(
                src_ref=src, dst_ref=dst,
                send_sem=send.at[target], recv_sem=recv.at[me],
                device_id={"sp": target}, device_id_type=MESH,
            ).wait_send()
        return carry

    lax.fori_loop(1, n_sp, drain, 0)
    for i in range(pieces):
        send_part(i).wait_send()
    for store in stores:
        store.wait()


def local_layer(
    n_sp,
    tokens, norm_gain, w_query, w_key, w_value, w_outgate, w_gatein, w_gateout, w_convin,
    w_igate, w_fgate, input_bias, forget_bias, forget_extra, init_memory, head_gain, conv_taps,
    out_memory, out_conv,
):
    own, width = tokens.shape[1:]
    count = 2 * own
    local_width = w_query.shape[1]
    heads, dh = init_memory.shape[1], init_memory.shape[3]
    nblocks = count // BLOCK
    slice_rows = heads * dh // n_sp
    vmem = pltpu.VMEM
    dma = pltpu.SemaphoreType.DMA
    scratch = [
        vmem((own, width), BF16),
        vmem((1, width), BF16),
        vmem((count, width), BF16),
        vmem((7, width, local_width), BF16),
        vmem((2 * local_width, width), BF16),
        vmem(w_igate.shape, BF16),
        vmem(w_fgate.shape, BF16),
        vmem((width, 128), BF16),
        vmem((7, count, local_width), BF16),
        vmem((count, 128), F32),
        vmem((count, heads), F32),
        vmem((1, 2 * heads), F32),
        vmem((1, 2 * heads), F32),
        vmem(conv_taps.shape, BF16),
        vmem((1, 2 * local_width), BF16),
        vmem((slice_rows, dh), F32),
        vmem((nblocks, heads, dh, BLOCK), BF16),
        vmem((nblocks, heads, dh, dh), BF16),
        vmem((6, nblocks * heads, BLOCK), F32),
        vmem((nblocks, BLOCK, BLOCK), F32),
        vmem((heads, dh, dh), F32),
        vmem((n_sp, slice_rows, dh), BF16),
        vmem((n_sp, slice_rows, dh), BF16),
        vmem((2 * heads, BLOCK), F32),
        vmem((n_sp, 2 * heads, BLOCK), F32),
        vmem((n_sp, slice_rows, dh), BF16),
        vmem((n_sp, slice_rows, dh), BF16),
        vmem((8, local_width), F32),
        vmem((count, local_width), F32),
        vmem((count, local_width), F32),
        vmem((count + 8, local_width), F32),
        vmem((count, 2 * local_width), BF16),
        vmem((own, width), BF16),
        vmem((own, width), BF16),
        dma((L_W + 7,)),
        dma, dma,
        dma((n_sp,)), dma((n_sp,)),
        dma((n_sp,)), dma((n_sp,)),
        dma((n_sp,)), dma((n_sp,)),
        dma, dma,
        dma((2,)), dma((2,)),
    ]
    return pl.pallas_call(
        functools.partial(kernel, n_sp),
        out_shape=jax.ShapeDtypeStruct(tokens.shape, BF16),
        in_specs=[pl.BlockSpec(memory_space=pl.ANY)] * 19,
        out_specs=pl.BlockSpec(memory_space=pl.ANY),
        scratch_shapes=scratch,
        compiler_params=pltpu.CompilerParams(
            collective_id=0, has_side_effects=True, vmem_limit_bytes=67043328
        ),
    )(
        tokens, norm_gain.reshape(1, -1),
        w_query, w_key, w_value, w_outgate, w_gatein, w_gateout, w_convin,
        w_igate, w_fgate, input_bias.reshape(1, -1), forget_bias.reshape(1, -1),
        forget_extra, init_memory, head_gain.reshape(1, -1), conv_taps, out_memory, out_conv,
    )


def solution(mesh):
    rows = P("fs", ("sp", "tp"), None)
    column, replicated = P(None, "tp"), P()
    return jax.shard_map(
        functools.partial(local_layer, mesh.shape["sp"]),
        mesh=mesh,
        in_specs=(
            rows, replicated,
            column, column, column, column, column, column, column,
            replicated, replicated, replicated, replicated,
            P("fs", "sp", "tp"), P("fs", "tp", None, None),
            replicated, replicated,
            P("tp", None), P("tp", None),
        ),
        out_specs=rows,
        check_vma=False,
    )
```

```python
import functools
import math

import jax
import jax.numpy as jnp
from jax import lax
from jax.experimental import pallas as pl
from jax.experimental.pallas import tpu as pltpu
from jax.sharding import PartitionSpec as P

MESH = pl.DeviceIdType.MESH
F32 = jnp.float32
BF16 = jnp.bfloat16
BLOCK = 128
EPSILON = 1e-06
LOWEST_LOG = -1e30

K_, V_, Q_, OG_, GI_, CI_, GO_ = range(7)
T_BIAS, T_KW, T_ALPHA, T_BETA, T_TOP, T_CARRY = range(6)
L_TOK, L_WIG, L_WFG, L_GAIN, L_FE, L_IB, L_FB, L_TAPS, L_HG, L_OM, L_OC, L_INIT, L_W = (
    0, 4, 5, 6, 7, 8, 9, 10, 11, 12, 13, 14, 16,
)


def kernel(
    n_sp,
    tokens, norm_gain, w_query, w_key, w_value, w_outgate, w_gatein, w_gateout, w_convin,
    w_igate, w_fgate, input_bias, forget_bias, forget_extra, init_memory, head_gain, conv_taps,
    out_memory, out_conv,
    out,
    tok, gain, x, w, wo, wig, wfg, proj, gates, fe, ib, fb, taps, hg, init,
    keys_t, prefix, table, cols, terms, seg, seg_in, scal, scal_in, state_out, state_in,
    rim_in, read, sig, prod, both, acc, part, part_in,
    lsem, tok_s, tok_r, gate_s, gate_r, seg_s, seg_r, scal_s, scal_r, st_s, st_r, rim_s, rim_r,
    out_s, out_r,
):
    own = tokens.shape[1]
    width = tokens.shape[2]
    count = 2 * own
    local_width = w_query.shape[1]
    heads = init_memory.shape[1]
    dh = init_memory.shape[3]
    nblocks = count // BLOCK
    half_blocks = nblocks // 2
    slice_rows = heads * dh // n_sp
    per_head = dh // slice_rows
    key_log = -0.5 * math.log(dh)
    me = lax.axis_index("sp")
    side = lax.axis_index("tp")
    other = 1 - side
    my_row = pl.multiple_of(side * own, own)
    peer_row = pl.multiple_of(other * own, own)
    my_block = side * half_blocks
    peer_block = other * half_blocks
    my_head = (me * slice_rows) // dh
    my_depth = pl.multiple_of(me * slice_rows - my_head * dh, slice_rows)
    my_lane = pl.multiple_of(side * local_width, local_width)
    my_rows = pl.ds(my_row, own)
    peer_rows = pl.ds(peer_row, own)

    def local(src, dst, index):
        return pltpu.make_async_copy(src, dst, lsem.at[index])

    weights = (w_key, w_value, w_query, w_outgate, w_gatein, w_convin, w_gateout)

    barrier = pltpu.get_barrier_semaphore()
    chunks = 4
    chunk_rows = own // chunks
    token_copies = [
        local(
            tokens.at[0, pl.ds(c * chunk_rows, chunk_rows), :],
            tok.at[pl.ds(c * chunk_rows, chunk_rows), :],
            L_TOK + c,
        )
        for c in range(chunks)
    ]
    gain_copy = local(norm_gain, gain, L_GAIN)
    narrow_copies = [local(w_igate, wig, L_WIG), local(w_fgate, wfg, L_WFG)]
    w_copies = [local(weights[p], w.at[p], L_W + p) for p in range(7)]
    gate_copies = [
        local(forget_extra.at[0], fe, L_FE),
        local(input_bias, ib, L_IB),
        local(forget_bias, fb, L_FB),
    ]
    head_copy = local(head_gain, hg, L_HG)
    taps_copy = local(conv_taps, taps, L_TAPS)
    init_copy = local(init_memory.at[0, my_head, pl.ds(my_depth, slice_rows), :], init, L_INIT)
    out_copies = [
        local(out_conv, wo.at[pl.ds(local_width, local_width), :], L_OC),
        local(out_memory, wo.at[pl.ds(0, local_width), :], L_OM),
    ]
    gain_copy.start()
    for copy in token_copies + narrow_copies + w_copies[:2]:
        copy.start()
    pl.semaphore_signal(barrier, inc=1, device_id={"tp": other}, device_id_type=MESH)

    def greet(k, carry):
        pl.semaphore_signal(
            barrier, inc=1, device_id={"sp": lax.rem(me + k, n_sp)}, device_id_type=MESH
        )
        return carry

    lax.fori_loop(1, n_sp, greet, 0)

    gain_copy.wait()
    gain_row = jnp.concatenate(
        [gain[i : i + 1, :] for i in range(gain.shape[0])], axis=1
    ).astype(F32)
    step_rows = 64
    for c in range(chunks):
        token_copies[c].wait()
        if c == chunks - 1:
            for copy in w_copies[2:] + gate_copies + [head_copy, taps_copy, init_copy]:
                copy.start()
            for copy in out_copies:
                copy.start()

        def norm_step(i, carry):
            rows = pl.multiple_of(c * chunk_rows + i * step_rows, step_rows)
            values = tok[pl.ds(rows, step_rows), :].astype(F32)
            scale = lax.rsqrt(jnp.mean(values * values, axis=-1, keepdims=True) + EPSILON)
            x[pl.ds(my_row + rows, step_rows), :] = (values * scale * gain_row).astype(BF16)
            return carry

        lax.fori_loop(0, chunk_rows // step_rows, norm_step, 0)

    def project(p, row):
        return jnp.dot(
            x[pl.ds(row, own), :], w[p], preferred_element_type=F32
        ).astype(BF16)

    def project_sig(row):
        value = project(OG_, row).astype(F32)
        gains = hg[...].astype(F32)
        gains = jnp.where(side == 0, gains[0:heads], gains[heads : 2 * heads])
        head_row = jnp.concatenate([gains[i : i + 1] for i in range(heads)], axis=1)
        sig[pl.ds(row, own), :] = head_row * jax.nn.sigmoid(value)

    def project_prod(row):
        value = project(CI_, row).astype(F32)
        prod[pl.ds(row + 16, own), :] = (
            proj[GI_, pl.ds(row, own), :].astype(F32) * value
        ).astype(BF16)

    for copy in narrow_copies:
        copy.wait()
    narrow = jnp.concatenate([wig[...], wfg[...]], axis=0)
    w_copies[K_].wait()
    gates[:, my_rows] = lax.dot_general(
        narrow, x[my_rows, :], (((1,), (1,)), ((), ())), preferred_element_type=F32
    )
    proj[K_, my_rows, :] = project(K_, my_row)

    pl.semaphore_wait(barrier, n_sp)
    peer = dict(device_id={"tp": other}, device_id_type=MESH)
    send_rows = pltpu.make_async_remote_copy(
        src_ref=x.at[my_rows, :], dst_ref=x.at[my_rows, :],
        send_sem=tok_s, recv_sem=tok_r, **peer,
    )
    take_rows = pltpu.make_async_remote_copy(
        src_ref=x.at[peer_rows, :], dst_ref=x.at[peer_rows, :],
        send_sem=tok_s, recv_sem=tok_r, **peer,
    )
    send_gates = pltpu.make_async_remote_copy(
        src_ref=gates.at[:, my_rows], dst_ref=gates.at[:, my_rows],
        send_sem=gate_s, recv_sem=gate_r, **peer,
    )
    take_gates = pltpu.make_async_remote_copy(
        src_ref=gates.at[:, peer_rows], dst_ref=gates.at[:, peer_rows],
        send_sem=gate_s, recv_sem=gate_r, **peer,
    )
    send_gates.start()
    send_rows.start()

    w_copies[V_].wait()
    w_copies[Q_].wait()
    proj[V_, my_rows, :] = project(V_, my_row)
    proj[Q_, my_rows, :] = project(Q_, my_row)
    w_copies[OG_].wait()
    w_copies[GI_].wait()
    head_copy.wait()
    for copy in gate_copies:
        copy.wait()
    take_gates.wait_recv()

    lanes = lax.broadcasted_iota(jnp.int32, (nblocks * heads, BLOCK), 1)
    head_rows = lax.broadcasted_iota(jnp.int32, (heads, BLOCK), 0)
    bias_in = jnp.zeros((heads, BLOCK), F32)
    bias_forget = jnp.zeros((heads, BLOCK), F32)
    for h in range(heads):
        for part_index in range(2):
            pick = (head_rows == h) & (side == part_index)
            c = part_index * heads + h
            bias_in = jnp.where(pick, ib[0:1, c : c + 1], bias_in)
            bias_forget = jnp.where(pick, fb[0:1, c : c + 1], bias_forget)
    ins, forgets = [], []
    for b in range(nblocks):
        at = slice(b * BLOCK, (b + 1) * BLOCK)
        pre = gates[:, at]
        ins.append(jnp.where(side == 0, pre[0:heads], pre[heads : 2 * heads]) + bias_in)
        forget = (
            jnp.where(side == 0, pre[2 * heads : 3 * heads], pre[3 * heads : 4 * heads])
            + bias_forget
        )
        forgets.append(
            jnp.minimum(forget, 0.0) - jnp.log1p(jnp.exp(-jnp.abs(forget))) + fe[:, at]
        )
    ins = jnp.concatenate(ins, axis=0)
    cumulative = jnp.concatenate(forgets, axis=0)
    shift = 1
    while shift < BLOCK:
        cumulative = cumulative + jnp.where(
            lanes >= shift, pltpu.roll(cumulative, shift, 1), 0.0
        )
        shift *= 2
    pair = ins - cumulative
    top = pair
    shift = 1
    while shift < BLOCK:
        top = jnp.maximum(top, jnp.where(lanes >= shift, pltpu.roll(top, shift, 1), top))
        shift *= 2
    total = jnp.broadcast_to(cumulative[:, BLOCK - 1 :], cumulative.shape)
    last_top = jnp.broadcast_to(top[:, BLOCK - 1 :], top.shape)
    log_scale = jnp.full((heads, BLOCK), LOWEST_LOG, F32)
    before = jnp.zeros((heads, BLOCK), F32)
    scales, befores, alphas, betas = [], [], [], []
    for b in range(nblocks):
        block_total = total[b * heads : (b + 1) * heads]
        block_top = block_total + last_top[b * heads : (b + 1) * heads]
        scales.append(log_scale)
        befores.append(before)
        merged = jnp.maximum(block_total + log_scale, block_top)
        alphas.append(block_total + log_scale - merged)
        betas.append(block_top - merged)
        log_scale = merged
        before = before + block_total
    scal[0:heads, :] = before
    scal[heads : 2 * heads, :] = log_scale
    scal_in[me] = scal[...]
    scales = jnp.concatenate(scales, axis=0)
    row_top = jnp.maximum(scales, top)
    table[T_BIAS] = pair + key_log
    table[T_KW] = jnp.exp(pair + key_log - last_top)
    table[T_ALPHA] = jnp.exp(jnp.concatenate(alphas, axis=0))
    table[T_BETA] = jnp.exp(jnp.concatenate(betas, axis=0))
    table[T_TOP] = row_top
    table[T_CARRY] = jnp.concatenate(befores, axis=0)
    carry_weight = jnp.exp(scales - row_top)
    fill = jnp.zeros((BLOCK - 2 * heads, BLOCK), F32)
    for b in range(nblocks):
        rows = slice(b * heads, (b + 1) * heads)
        cols[b] = jnp.concatenate([row_top[rows], carry_weight[rows], fill], axis=0).T
    project_sig(my_row)
    proj[GI_, my_rows, :] = project(GI_, my_row)

    def send_scales(k, carry):
        target = lax.rem(me + k, n_sp)
        pltpu.make_async_remote_copy(
            src_ref=scal, dst_ref=scal_in.at[me],
            send_sem=scal_s.at[target], recv_sem=scal_r.at[me],
            device_id={"sp": target}, device_id_type=MESH,
        ).start()
        return carry

    lax.fori_loop(1, n_sp, send_scales, 0)

    def block_terms(first):
        for i in range(half_blocks):
            b = first + i
            rows = pl.ds(pl.multiple_of(b * BLOCK, BLOCK), BLOCK)
            for h in range(heads):
                hs = slice(h * dh, (h + 1) * dh)
                turned = proj[K_, rows, hs].T
                keys_t[b, h] = turned
                weighted = (
                    turned.astype(F32) * table[T_KW, pl.ds(b * heads + h, 1), :]
                ).astype(BF16)
                terms[b, h] = jnp.dot(weighted, proj[V_, rows, hs], preferred_element_type=F32)

    take_rows.wait_recv()
    block_terms(my_block)
    proj[K_, peer_rows, :] = project(K_, peer_row)
    proj[V_, peer_rows, :] = project(V_, peer_row)

    w_copies[CI_].wait()
    w_copies[GO_].wait()
    block_terms(peer_block)
    for h in range(heads):
        held = jnp.zeros((dh, dh), F32)
        for b in range(nblocks):
            at = pl.ds(b * heads + h, 1)
            prefix[b, h] = held.astype(BF16)
            held = table[T_ALPHA, at, :] * held + table[T_BETA, at, :] * terms[b, h]
        for piece in range(per_head):
            seg[h * per_head + piece] = held[
                piece * slice_rows : (piece + 1) * slice_rows, :
            ].astype(BF16)
    project_prod(my_row)

    seg_in[me] = seg[me]

    def send_segment(k, carry):
        target = lax.rem(me + k, n_sp)
        pltpu.make_async_remote_copy(
            src_ref=seg.at[target], dst_ref=seg_in.at[me],
            send_sem=seg_s.at[target], recv_sem=seg_r.at[me],
            device_id={"sp": target}, device_id_type=MESH,
        ).start()
        return carry

    lax.fori_loop(1, n_sp, send_segment, 0)

    proj[GI_, peer_rows, :] = project(GI_, peer_row)
    project_prod(peer_row)
    following = lax.rem(me + 1, n_sp)
    rim = pltpu.make_async_remote_copy(
        src_ref=prod.at[pl.ds(count, 16), :], dst_ref=rim_in,
        send_sem=rim_s, recv_sem=rim_r,
        device_id={"sp": following}, device_id_type=MESH,
    )
    rim.start()

    t_index = lax.broadcasted_iota(jnp.int32, (BLOCK, BLOCK), 0)
    s_index = lax.broadcasted_iota(jnp.int32, (BLOCK, BLOCK), 1)
    causal = s_index <= t_index

    def read_blocks(first):
        for i in range(half_blocks):
            b = first + i
            rows = pl.ds(pl.multiple_of(b * BLOCK, BLOCK), BLOCK)
            columns = cols[b]
            for h in range(heads):
                at = pl.ds(b * heads + h, 1)
                hs = slice(h * dh, (h + 1) * dh)
                query = proj[Q_, rows, hs]
                scores = jnp.dot(query, keys_t[b, h], preferred_element_type=F32)
                log_weight = jnp.where(
                    causal, table[T_BIAS, at, :] - columns[:, h : h + 1], -jnp.inf
                )
                weighted = (jnp.exp(log_weight) * scores).astype(BF16)
                read[rows, hs] = jnp.dot(
                    weighted, proj[V_, rows, hs], preferred_element_type=F32
                ) + columns[:, heads + h : heads + h + 1] * jnp.dot(
                    query, prefix[b, h], preferred_element_type=F32
                )

    read_blocks(my_block)
    proj[Q_, peer_rows, :] = project(Q_, peer_row)
    project_sig(peer_row)

    read_blocks(peer_block)
    proj[GO_, my_rows, :] = project(GO_, my_row)
    proj[GO_, peer_rows, :] = project(GO_, peer_row)

    def wait_from(src, dst, send, recv):
        def step(k, carry):
            source = lax.rem(me + k, n_sp)
            pltpu.make_async_remote_copy(
                src_ref=src.at[source] if src is not scal else src,
                dst_ref=dst.at[source],
                send_sem=send.at[source], recv_sem=recv.at[source],
                device_id={"sp": source}, device_id_type=MESH,
            ).wait_recv()
            return carry

        lax.fori_loop(1, n_sp, step, 0)

    init_copy.wait()
    wait_from(scal, scal_in, scal_s, scal_r)
    wait_from(seg, seg_in, seg_s, seg_r)

    state = init[...]
    state_log = jnp.zeros((1, BLOCK), F32)
    for i in range(n_sp):
        state_out[i] = state.astype(BF16)
        if i == n_sp - 1:
            break
        span = scal_in[i, pl.ds(my_head, 1), :]
        span_top = scal_in[i, pl.ds(heads + my_head, 1), :]
        merged = jnp.maximum(span + state_log, span_top)
        state = (
            jnp.exp(span + state_log - merged) * state
            + jnp.exp(span_top - merged) * seg_in[i].astype(F32)
        )
        state_log = merged
    state_in[me] = state_out[me]

    def send_state(k, carry):
        target = lax.rem(me + k, n_sp)
        pltpu.make_async_remote_copy(
            src_ref=state_out.at[target], dst_ref=state_in.at[me],
            send_sem=st_s.at[target], recv_sem=st_r.at[me],
            device_id={"sp": target}, device_id_type=MESH,
        ).start()
        return carry

    lax.fori_loop(1, n_sp, send_state, 0)

    taps_copy.wait()
    pltpu.make_async_remote_copy(
        src_ref=prod.at[pl.ds(count, 16), :], dst_ref=rim_in,
        send_sem=rim_s, recv_sem=rim_r,
        device_id={"sp": following}, device_id_type=MESH,
    ).wait_recv()
    for copy in out_copies:
        copy.wait()
    prod[0:16, :] = jnp.where(me == 0, jnp.zeros_like(rim_in), rim_in[...])
    tap_rows = taps[:, pl.ds(my_lane, local_width)].astype(F32)
    conv_rows = 64

    def convolve(first):
        for i in range(own // conv_rows):
            row = pl.multiple_of(first + i * conv_rows, conv_rows)
            window = prod[pl.ds(row, conv_rows + 16), :].astype(F32)
            mixed = window[14 : 14 + conv_rows] * tap_rows[0:1]
            mixed = mixed + window[15 : 15 + conv_rows] * tap_rows[1:2]
            mixed = mixed + window[16 : 16 + conv_rows] * tap_rows[2:3]
            both[pl.ds(row, conv_rows), local_width:] = (
                proj[GO_, pl.ds(row, conv_rows), :].astype(F32) * mixed
            ).astype(BF16)

    convolve(peer_row)
    acc[...] = jnp.dot(
        both[peer_rows, local_width:], wo[pl.ds(local_width, local_width), :],
        preferred_element_type=F32,
    )
    convolve(my_row)

    start_log = jnp.zeros((heads, BLOCK), F32)
    for i in range(n_sp - 1):
        merged = jnp.maximum(scal_in[i, 0:heads, :] + start_log, scal_in[i, heads : 2 * heads, :])
        start_log = jnp.where(i < me, merged, start_log)
    carried_log = table[T_CARRY] + jnp.concatenate([start_log] * nblocks, axis=0)
    new_top = jnp.maximum(table[T_TOP], carried_log)
    keep = jnp.exp(table[T_TOP] - new_top)
    bring = jnp.exp(carried_log - new_top)
    for b in range(nblocks):
        rows = slice(b * heads, (b + 1) * heads)
        cols[b] = jnp.concatenate([keep[rows], bring[rows], fill], axis=0).T

    wait_from(state_out, state_in, st_s, st_r)

    pieces = 2
    piece_rows = own // pieces

    def finish(row):
        for i in range(piece_rows // BLOCK):
            b = row // BLOCK + i
            rows = pl.ds(pl.multiple_of(b * BLOCK, BLOCK), BLOCK)
            columns = cols[b]
            for h in range(heads):
                hs = slice(h * dh, (h + 1) * dh)
                start = state_in[h * per_head : (h + 1) * per_head].reshape(dh, dh)
                readout = columns[:, h : h + 1] * read[rows, hs] + columns[
                    :, heads + h : heads + h + 1
                ] * jnp.dot(proj[Q_, rows, hs], start, preferred_element_type=F32)
                normalized = readout * lax.rsqrt(
                    jnp.mean(readout * readout, axis=-1, keepdims=True) + EPSILON
                )
                both[rows, hs] = (normalized * sig[rows, hs]).astype(BF16)

    def send_part(i):
        return pltpu.make_async_remote_copy(
            src_ref=part.at[pl.ds(i * piece_rows, piece_rows), :],
            dst_ref=part_in.at[pl.ds(i * piece_rows, piece_rows), :],
            send_sem=out_s.at[i], recv_sem=out_r.at[i],
            device_id={"tp": other}, device_id_type=MESH,
        )

    finish(peer_row)
    for i in range(pieces):
        rows = pl.ds(i * piece_rows, piece_rows)
        if i + 1 < pieces:
            finish(peer_row + (i + 1) * piece_rows)
        else:
            finish(my_row)
        part[rows, :] = (
            acc[rows, :]
            + jnp.dot(
                both[pl.ds(peer_row + i * piece_rows, piece_rows), 0:local_width],
                wo[pl.ds(0, local_width), :],
                preferred_element_type=F32,
            )
        ).astype(BF16)
        send_part(i).start()

    for i in range(pieces):
        if i + 1 < pieces:
            finish(my_row + (i + 1) * piece_rows)
        mine = jnp.dot(
            both[pl.ds(my_row + i * piece_rows, piece_rows), :], wo[...],
            preferred_element_type=F32,
        ).astype(BF16)
        rows = pl.ds(i * piece_rows, piece_rows)
        send_part(i).wait_recv()
        out[0, rows, :] = (mine.astype(F32) + part_in[rows, :].astype(F32)).astype(BF16)

    send_rows.wait_send()
    send_gates.wait_send()
    rim.wait_send()

    def drain(k, carry):
        target = lax.rem(me + k, n_sp)
        for src, send, recv, dst in (
            (scal, scal_s, scal_r, scal_in.at[me]),
            (seg.at[target], seg_s, seg_r, seg_in.at[me]),
            (state_out.at[target], st_s, st_r, state_in.at[me]),
        ):
            pltpu.make_async_remote_copy(
                src_ref=src, dst_ref=dst,
                send_sem=send.at[target], recv_sem=recv.at[me],
                device_id={"sp": target}, device_id_type=MESH,
            ).wait_send()
        return carry

    lax.fori_loop(1, n_sp, drain, 0)
    for i in range(pieces):
        send_part(i).wait_send()


def store_kernel(src, dst, sems):
    rows = src.shape[1] // 4
    copies = [
        pltpu.make_async_copy(
            src.at[0, pl.ds(i * rows, rows), :], dst.at[0, pl.ds(i * rows, rows), :], sems.at[i]
        )
        for i in range(4)
    ]
    for copy in copies:
        copy.start()
    for copy in copies:
        copy.wait()


def local_layer(
    n_sp,
    tokens, norm_gain, w_query, w_key, w_value, w_outgate, w_gatein, w_gateout, w_convin,
    w_igate, w_fgate, input_bias, forget_bias, forget_extra, init_memory, head_gain, conv_taps,
    out_memory, out_conv,
):
    own, width = tokens.shape[1:]
    count = 2 * own
    local_width = w_query.shape[1]
    heads, dh = init_memory.shape[1], init_memory.shape[3]
    nblocks = count // BLOCK
    slice_rows = heads * dh // n_sp
    vmem = pltpu.VMEM
    dma = pltpu.SemaphoreType.DMA
    scratch = [
        vmem((own, width), BF16),
        vmem((width // 128, 128), BF16),
        vmem((count, width), BF16),
        vmem((7, width, local_width), BF16),
        vmem((2 * local_width, width), BF16),
        vmem((2 * heads, width), BF16),
        vmem((2 * heads, width), BF16),
        vmem((7, count, local_width), BF16),
        vmem((4 * heads, count), F32),
        vmem((heads, count), F32),
        vmem((1, 2 * heads), F32),
        vmem((1, 2 * heads), F32),
        vmem(conv_taps.shape, BF16),
        vmem((2 * heads, dh), BF16),
        vmem((slice_rows, dh), F32),
        vmem((nblocks, heads, dh, BLOCK), BF16),
        vmem((nblocks, heads, dh, dh), BF16),
        vmem((6, nblocks * heads, BLOCK), F32),
        vmem((nblocks, BLOCK, BLOCK), F32),
        vmem((nblocks, heads, dh, dh), F32),
        vmem((n_sp, slice_rows, dh), BF16),
        vmem((n_sp, slice_rows, dh), BF16),
        vmem((2 * heads, BLOCK), F32),
        vmem((n_sp, 2 * heads, BLOCK), F32),
        vmem((n_sp, slice_rows, dh), BF16),
        vmem((n_sp, slice_rows, dh), BF16),
        vmem((16, local_width), BF16),
        vmem((count, local_width), F32),
        vmem((count, local_width), F32),
        vmem((count + 16, local_width), BF16),
        vmem((count, 2 * local_width), BF16),
        vmem((own, width), F32),
        vmem((own, width), BF16),
        vmem((own, width), BF16),
        dma((L_W + 7,)),
        dma, dma, dma, dma,
        dma((n_sp,)), dma((n_sp,)),
        dma((n_sp,)), dma((n_sp,)),
        dma((n_sp,)), dma((n_sp,)),
        dma, dma,
        dma((2,)), dma((2,)),
    ]
    rows = pl.pallas_call(
        functools.partial(kernel, n_sp),
        out_shape=vmem(tokens.shape, BF16),
        in_specs=[pl.BlockSpec(memory_space=pl.ANY)] * 19,
        out_specs=pl.BlockSpec(memory_space=pltpu.VMEM),
        scratch_shapes=scratch,
        compiler_params=pltpu.CompilerParams(
            collective_id=0, has_side_effects=True, vmem_limit_bytes=58 * 1024 * 1024
        ),
    )(
        tokens, norm_gain.reshape(-1, 128),
        w_query, w_key, w_value, w_outgate, w_gatein, w_gateout, w_convin,
        w_igate.T, w_fgate.T, input_bias.reshape(1, -1), forget_bias.reshape(1, -1),
        jnp.swapaxes(forget_extra, 1, 2), init_memory, head_gain.reshape(-1, dh), conv_taps,
        out_memory, out_conv,
    )
    return pl.pallas_call(
        store_kernel,
        out_shape=jax.ShapeDtypeStruct(tokens.shape, BF16),
        in_specs=[pl.BlockSpec(memory_space=pltpu.VMEM)],
        out_specs=pl.BlockSpec(memory_space=pl.ANY),
        scratch_shapes=[dma((4,))],
    )(pltpu.with_memory_space_constraint(rows, pltpu.VMEM))


def solution(mesh):
    rows = P("fs", ("sp", "tp"), None)
    column, replicated = P(None, "tp"), P()
    return jax.shard_map(
        functools.partial(local_layer, mesh.shape["sp"]),
        mesh=mesh,
        in_specs=(
            rows, replicated,
            column, column, column, column, column, column, column,
            replicated, replicated, replicated, replicated,
            P("fs", "sp", "tp"), P("fs", "tp", None, None),
            replicated, replicated,
            P("tp", None), P("tp", None),
        ),
        out_specs=rows,
        check_vma=False,
    )
```

```python
import functools
import math

import jax
import jax.numpy as jnp
from jax import lax
from jax.experimental import pallas as pl
from jax.experimental.pallas import tpu as pltpu
from jax.sharding import PartitionSpec as P

MESH = pl.DeviceIdType.MESH
F32 = jnp.float32
BF16 = jnp.bfloat16
BLOCK = 128
EPSILON = 1e-06
LOWEST_LOG = -1e30

K_, V_, Q_, OG_, GI_, CI_, GO_ = range(7)
T_BIAS, T_KW, T_ALPHA, T_BETA, T_TOP, T_CARRY = range(6)
L_TOK, L_WIG, L_WFG, L_GAIN, L_FE, L_IB, L_FB, L_TAPS, L_HG, L_OM, L_OC, L_INIT, L_W = (
    0, 4, 5, 6, 7, 8, 9, 10, 11, 12, 13, 14, 16,
)


def kernel(
    n_sp,
    tokens, norm_gain, w_query, w_key, w_value, w_outgate, w_gatein, w_gateout, w_convin,
    w_igate, w_fgate, input_bias, forget_bias, forget_extra, init_memory, head_gain, conv_taps,
    out_memory, out_conv,
    out,
    tok, gain, w_all, wom, woc, wig, wfg, gates, fe, ib, fb, taps, hg, init,
    x_own, x_peer, proj_own, proj_peer, sig_own, sig_peer, read_own, read_peer,
    conv_own, conv_peer, conv_in, acc, mem_0, mem_1, mem_2, mem_3, mem_in, wom_in, woc_in,
    keys, table, cols, cols_in, terms, seg, seg_in, scal, scal_in, state_out, state_in,
    rim_in, prod,
    ready, lsem, tok_s, tok_r, gate_s, gate_r, seg_s, seg_r, scal_s, scal_r, st_s, st_r,
    rim_s, rim_r, ow_s, ow_r, conv_s, conv_r, mem_s, mem_r,
):
    own = tokens.shape[1]
    count = 2 * own
    local_width = w_query.shape[1]
    heads = init_memory.shape[1]
    dh = init_memory.shape[3]
    nblocks = count // BLOCK
    half_blocks = nblocks // 2
    slice_rows = heads * dh // n_sp
    per_head = dh // slice_rows
    key_log = -0.5 * math.log(dh)
    me = lax.axis_index("sp")
    side = lax.axis_index("tp")
    other = 1 - side
    my_row = pl.multiple_of(side * own, own)
    peer_row = pl.multiple_of(other * own, own)
    my_block = side * half_blocks
    peer_block = other * half_blocks
    my_head = (me * slice_rows) // dh
    my_depth = pl.multiple_of(me * slice_rows - my_head * dh, slice_rows)
    my_lane = pl.multiple_of(side * local_width, local_width)
    my_rows = pl.ds(my_row, own)
    peer_rows = pl.ds(peer_row, own)

    def local(src, dst, index):
        return pltpu.make_async_copy(src, dst, lsem.at[index])

    def sp(target):
        return dict(device_id={"sp": target}, device_id_type=MESH)

    peer = dict(device_id={"tp": other}, device_id_type=MESH)
    weights = (w_key, w_value, w_query, w_outgate, w_gatein, w_convin, w_gateout)

    barrier = pltpu.get_barrier_semaphore()
    chunks = 4
    chunk_rows = own // chunks
    token_copies = [
        local(
            tokens.at[0, pl.ds(c * chunk_rows, chunk_rows), :],
            tok.at[pl.ds(c * chunk_rows, chunk_rows), :],
            L_TOK + c,
        )
        for c in range(chunks)
    ]
    gain_copy = local(norm_gain, gain, L_GAIN)
    narrow_copies = [local(w_igate, wig, L_WIG), local(w_fgate, wfg, L_WFG)]
    w_copies = [local(weights[p], w_all[p], L_W + p) for p in range(7)]
    gate_copies = [
        local(forget_extra.at[0], fe, L_FE),
        local(input_bias, ib, L_IB),
        local(forget_bias, fb, L_FB),
    ]
    head_copy = local(head_gain, hg, L_HG)
    taps_copy = local(conv_taps, taps, L_TAPS)
    init_copy = local(init_memory.at[0, my_head, pl.ds(my_depth, slice_rows), :], init, L_INIT)
    out_copies = [local(out_conv, woc, L_OC), local(out_memory, wom, L_OM)]
    gain_copy.start()
    for copy in token_copies + narrow_copies + w_copies[:2] + gate_copies:
        copy.start()
    pl.semaphore_signal(barrier, inc=1, **peer)

    def greet(k, carry):
        pl.semaphore_signal(barrier, inc=1, **sp(k))
        return carry

    lax.fori_loop(me + 1, n_sp, greet, 0)

    gain_copy.wait()
    gain_row = jnp.concatenate(
        [gain[i : i + 1, :] for i in range(gain.shape[0])], axis=1
    ).astype(F32)
    step_rows = 64
    for c in range(chunks):
        token_copies[c].wait()

        def norm_step(i, carry):
            rows = pl.ds(pl.multiple_of(c * chunk_rows + i * step_rows, step_rows), step_rows)
            values = tok[rows, :].astype(F32)
            scale = lax.rsqrt(jnp.mean(values * values, axis=-1, keepdims=True) + EPSILON)
            x_own[rows, :] = (values * scale * gain_row).astype(BF16)
            return carry

        lax.fori_loop(0, chunk_rows // step_rows, norm_step, 0)

    for copy in narrow_copies:
        copy.wait()
    narrow = jnp.concatenate([wig[...], wfg[...]], axis=0)
    gates[:, my_rows] = lax.dot_general(
        narrow, x_own[...], (((1,), (1,)), ((), ())), preferred_element_type=F32
    )

    pl.semaphore_wait(barrier, me + 1)
    send_rows = pltpu.make_async_remote_copy(
        src_ref=x_own, dst_ref=x_peer, send_sem=tok_s, recv_sem=tok_r, **peer
    )
    send_gates = pltpu.make_async_remote_copy(
        src_ref=gates.at[:, my_rows], dst_ref=gates.at[:, my_rows],
        send_sem=gate_s, recv_sem=gate_r, **peer,
    )
    take_gates = pltpu.make_async_remote_copy(
        src_ref=gates.at[:, peer_rows], dst_ref=gates.at[:, peer_rows],
        send_sem=gate_s, recv_sem=gate_r, **peer,
    )
    send_gates.start()
    send_rows.start()

    def answer(k, carry):
        pl.semaphore_signal(ready, inc=1, **sp(k))
        return carry

    lax.fori_loop(0, me, answer, 0)

    pieces = 2
    piece_rows = own // pieces
    spans = [slice(i * piece_rows, (i + 1) * piece_rows) for i in range(pieces)]

    def project(p, rows, dst):
        for at in spans:
            dst[p][at, :] = jnp.dot(
                rows[at, :], w_all[p][...], preferred_element_type=F32
            ).astype(BF16)

    def head_gains():
        gains = hg[...].astype(F32)
        gains = jnp.where(side == 0, gains[0:heads], gains[heads : 2 * heads])
        return jnp.concatenate([gains[i : i + 1] for i in range(heads)], axis=1)

    def project_sig(rows, dst):
        head_row = head_gains()
        for at in spans:
            value = jnp.dot(
                rows[at, :], w_all[OG_][...], preferred_element_type=F32
            ).astype(BF16)
            dst[at, :] = head_row * jax.nn.sigmoid(value.astype(F32))

    def piece_of(p, rows, dst, i):
        at = spans[i]
        dst[p][at, :] = jnp.dot(
            rows[at, :], w_all[p][...], preferred_element_type=F32
        ).astype(BF16)

    def prod_piece(rows, proj, row, i):
        at = spans[i]
        value = jnp.dot(rows[at, :], w_all[CI_][...], preferred_element_type=F32).astype(BF16)
        prod[pl.ds(row + 16 + i * piece_rows, piece_rows), :] = (
            proj[GI_][at, :].astype(F32) * value.astype(F32)
        ).astype(BF16)

    w_copies[K_].wait()
    w_copies[V_].wait()
    for copy in w_copies[2:4] + [head_copy] + w_copies[4:]:
        copy.start()
    for copy in [taps_copy, init_copy] + out_copies:
        copy.start()
    project(K_, x_own, proj_own)
    project(V_, x_own, proj_own)
    w_copies[Q_].wait()
    w_copies[OG_].wait()
    head_copy.wait()
    for copy in gate_copies:
        copy.wait()
    take_gates.wait_recv()

    lanes = lax.broadcasted_iota(jnp.int32, (nblocks * heads, BLOCK), 1)
    head_rows = lax.broadcasted_iota(jnp.int32, (heads, BLOCK), 0)
    bias_in = jnp.zeros((heads, BLOCK), F32)
    bias_forget = jnp.zeros((heads, BLOCK), F32)
    for h in range(heads):
        for part_index in range(2):
            pick = (head_rows == h) & (side == part_index)
            c = part_index * heads + h
            bias_in = jnp.where(pick, ib[0:1, c : c + 1], bias_in)
            bias_forget = jnp.where(pick, fb[0:1, c : c + 1], bias_forget)
    ins, forgets = [], []
    for b in range(nblocks):
        at = slice(b * BLOCK, (b + 1) * BLOCK)
        pre = gates[:, at]
        ins.append(jnp.where(side == 0, pre[0:heads], pre[heads : 2 * heads]) + bias_in)
        forget = (
            jnp.where(side == 0, pre[2 * heads : 3 * heads], pre[3 * heads : 4 * heads])
            + bias_forget
        )
        forgets.append(
            jnp.minimum(forget, 0.0) - jnp.log1p(jnp.exp(-jnp.abs(forget))) + fe[:, at]
        )
    ins = jnp.concatenate(ins, axis=0)
    cumulative = jnp.concatenate(forgets, axis=0)
    shift = 1
    while shift < BLOCK:
        cumulative = cumulative + jnp.where(
            lanes >= shift, pltpu.roll(cumulative, shift, 1), 0.0
        )
        shift *= 2
    pair = ins - cumulative
    top = pair
    shift = 1
    while shift < BLOCK:
        top = jnp.maximum(top, jnp.where(lanes >= shift, pltpu.roll(top, shift, 1), top))
        shift *= 2
    total = jnp.broadcast_to(cumulative[:, BLOCK - 1 :], cumulative.shape)
    last_top = jnp.broadcast_to(top[:, BLOCK - 1 :], top.shape)
    log_scale = jnp.full((heads, BLOCK), LOWEST_LOG, F32)
    before = jnp.zeros((heads, BLOCK), F32)
    scales, befores, alphas, betas = [], [], [], []
    for b in range(nblocks):
        block_total = total[b * heads : (b + 1) * heads]
        block_top = block_total + last_top[b * heads : (b + 1) * heads]
        scales.append(log_scale)
        befores.append(before)
        merged = jnp.maximum(block_total + log_scale, block_top)
        alphas.append(block_total + log_scale - merged)
        betas.append(block_top - merged)
        log_scale = merged
        before = before + block_total
    scal[0:heads, :] = before
    scal[heads : 2 * heads, :] = log_scale
    scal_in[me] = scal[...]
    scales = jnp.concatenate(scales, axis=0)
    row_top = jnp.maximum(scales, top)
    table[T_BIAS] = pair + key_log
    table[T_KW] = jnp.exp(pair + key_log - last_top)
    table[T_ALPHA] = jnp.exp(jnp.concatenate(alphas, axis=0))
    table[T_BETA] = jnp.exp(jnp.concatenate(betas, axis=0))
    table[T_TOP] = row_top
    table[T_CARRY] = jnp.concatenate(befores, axis=0)
    carry_weight = jnp.exp(scales - row_top)
    fill = jnp.zeros((BLOCK - 2 * heads, BLOCK), F32)
    for b in range(nblocks):
        rows = slice(b * heads, (b + 1) * heads)
        cols[b] = jnp.concatenate([row_top[rows], carry_weight[rows], fill], axis=0).T
    project(Q_, x_own, proj_own)
    project_sig(x_own, sig_own)

    def weigh_keys(proj, first):
        weighted = []
        for i in range(half_blocks):
            rows = slice(i * BLOCK, (i + 1) * BLOCK)
            b = first + i
            for h in range(heads):
                turned = proj[K_][rows, h * dh : (h + 1) * dh].T
                keys[b, h, :, 0:BLOCK] = turned
                weighted.append(
                    (turned.astype(F32) * table[T_KW, pl.ds(b * heads + h, 1), :]).astype(BF16)
                )
        return weighted

    def block_terms(weighted, proj, first):
        for i in range(half_blocks):
            rows = slice(i * BLOCK, (i + 1) * BLOCK)
            for h in range(heads):
                terms[first + i, h] = jnp.dot(
                    weighted[i * heads + h], proj[V_][rows, h * dh : (h + 1) * dh],
                    preferred_element_type=F32,
                )

    w_copies[GI_].wait()
    w_copies[CI_].wait()
    w_copies[GO_].wait()
    take_rows = pltpu.make_async_remote_copy(
        src_ref=x_own, dst_ref=x_peer, send_sem=tok_s, recv_sem=tok_r, **peer
    )
    take_rows.wait_recv()
    out_weights = [
        pltpu.make_async_remote_copy(
            src_ref=src, dst_ref=dst, send_sem=ow_s.at[i], recv_sem=ow_r.at[i], **peer
        )
        for i, (src, dst) in enumerate(((out_conv, woc_in), (out_memory, wom_in)))
    ]
    for copy in out_weights:
        copy.start()
    weighted_own = weigh_keys(proj_own, my_block)
    project(K_, x_peer, proj_peer)
    block_terms(weighted_own, proj_own, my_block)
    weighted_peer = weigh_keys(proj_peer, peer_block)
    project(V_, x_peer, proj_peer)
    block_terms(weighted_peer, proj_peer, peer_block)

    @pl.when(me < n_sp - 1)
    def _():
        pl.semaphore_wait(ready, n_sp - 1 - me)

    for h in range(heads):
        held = jnp.zeros((dh, dh), F32)
        for b in range(nblocks):
            at = pl.ds(b * heads + h, 1)
            keys[b, h, :, BLOCK:] = held.astype(BF16)
            held = table[T_ALPHA, at, :] * held + table[T_BETA, at, :] * terms[b, h]
        for piece in range(per_head):
            seg[h * per_head + piece] = held[
                piece * slice_rows : (piece + 1) * slice_rows, :
            ].astype(BF16)
    seg_in[me] = seg[me]

    def segment_copies(target):
        return (
            pltpu.make_async_remote_copy(
                src_ref=scal, dst_ref=scal_in.at[me],
                send_sem=scal_s.at[target], recv_sem=scal_r.at[me], **sp(target),
            ),
            pltpu.make_async_remote_copy(
                src_ref=seg.at[target], dst_ref=seg_in.at[me],
                send_sem=seg_s.at[target], recv_sem=seg_r.at[me], **sp(target),
            ),
        )

    for k in range(1, n_sp):
        for copy in segment_copies(lax.rem(me + k, n_sp)):
            copy.start()
    project(GI_, x_own, proj_own)

    t_index = lax.broadcasted_iota(jnp.int32, (BLOCK, BLOCK), 0)
    s_index = lax.broadcasted_iota(jnp.int32, (BLOCK, BLOCK), 1)
    causal = s_index <= t_index

    def read_blocks(proj, read, first, chunks):
        def scores_of(i):
            rows = slice(i * BLOCK, (i + 1) * BLOCK)
            return [
                jnp.dot(
                    proj[Q_][rows, h * dh : (h + 1) * dh], keys[first + i, h],
                    preferred_element_type=F32,
                )
                for h in range(heads)
            ]

        def weigh(i, raw):
            columns = cols[first + i]
            weighted, carried = [], []
            for h in range(heads):
                log_weight = jnp.where(
                    causal,
                    table[T_BIAS, pl.ds((first + i) * heads + h, 1), :] - columns[:, h : h + 1],
                    -jnp.inf,
                )
                weighted.append((jnp.exp(log_weight) * raw[h][:, 0:BLOCK]).astype(BF16))
                carried.append(columns[:, heads + h : heads + h + 1] * raw[h][:, BLOCK:])
            return weighted, carried

        def read_out(i, weighted, carried):
            rows = slice(i * BLOCK, (i + 1) * BLOCK)
            for h in range(heads):
                hs = slice(h * dh, (h + 1) * dh)
                read[rows, hs] = carried[h] + jnp.dot(
                    weighted[h], proj[V_][rows, hs], preferred_element_type=F32
                )

        raw = scores_of(0)
        for i in range(half_blocks):
            parts = weigh(i, raw)
            chunks[i]()
            if i + 1 < half_blocks:
                raw = scores_of(i + 1)
            read_out(i, *parts)
        for chunk in chunks[half_blocks:]:
            chunk()

    read_blocks(
        proj_own, read_own, my_block,
        [
            lambda: prod_piece(x_own, proj_own, my_row, 0),
            lambda: prod_piece(x_own, proj_own, my_row, 1),
            lambda: piece_of(GI_, x_peer, proj_peer, 0),
            lambda: piece_of(GI_, x_peer, proj_peer, 1),
        ],
    )
    project(Q_, x_peer, proj_peer)

    def owner_step():
        init_copy.wait()

        def wait_segment(k, carry):
            source = lax.rem(me + k, n_sp)
            pltpu.make_async_remote_copy(
                src_ref=scal, dst_ref=scal_in.at[source],
                send_sem=scal_s.at[source], recv_sem=scal_r.at[source], **sp(source),
            ).wait_recv()
            pltpu.make_async_remote_copy(
                src_ref=seg.at[source], dst_ref=seg_in.at[source],
                send_sem=seg_s.at[source], recv_sem=seg_r.at[source], **sp(source),
            ).wait_recv()
            return carry

        lax.fori_loop(1, n_sp, wait_segment, 0)
        state = init[...]
        state_log = jnp.zeros((1, BLOCK), F32)
        for i in range(n_sp):
            state_out[i] = state.astype(BF16)
            if i == n_sp - 1:
                break
            span = scal_in[i, pl.ds(my_head, 1), :]
            span_top = scal_in[i, pl.ds(heads + my_head, 1), :]
            merged = jnp.maximum(span + state_log, span_top)
            state = (
                jnp.exp(span + state_log - merged) * state
                + jnp.exp(span_top - merged) * seg_in[i].astype(F32)
            )
            state_log = merged
        state_in[me] = state_out[me]

        def send_state(k, carry):
            target = lax.rem(me + k, n_sp)
            pltpu.make_async_remote_copy(
                src_ref=state_out.at[target], dst_ref=state_in.at[me],
                send_sem=st_s.at[target], recv_sem=st_r.at[me], **sp(target),
            ).start()
            return carry

        lax.fori_loop(1, n_sp, send_state, 0)

    along_x, along_z = lax.rem(me, 4), me // 4
    lateness = 2 * along_z + jnp.where(along_x == 3, 3, 2 * along_x)
    late = lateness >= 6
    early = lateness < 4
    pl.when(late)(owner_step)

    prod_piece(x_peer, proj_peer, peer_row, 0)
    prod_piece(x_peer, proj_peer, peer_row, 1)

    def rim_copy(target):
        return pltpu.make_async_remote_copy(
            src_ref=prod.at[pl.ds(count, 16), :], dst_ref=rim_in,
            send_sem=rim_s, recv_sem=rim_r, **sp(target),
        )

    last = me == n_sp - 1

    @pl.when(jnp.logical_not(last))
    def _():
        rim_copy(me + 1).start()

    pl.when(jnp.logical_not(late | early))(owner_step)

    read_blocks(
        proj_peer, read_peer, peer_block,
        [
            lambda: piece_of(GO_, x_own, proj_own, 0),
            lambda: piece_of(GO_, x_own, proj_own, 1),
            lambda: piece_of(GO_, x_peer, proj_peer, 0),
            lambda: piece_of(GO_, x_peer, proj_peer, 1),
        ],
    )

    pl.when(early)(owner_step)

    taps_copy.wait()
    for copy in out_copies:
        copy.wait()

    @pl.when(me == 0)
    def _():
        rim_in[...] = jnp.zeros_like(rim_in)

    @pl.when(me > 0)
    def _():
        rim_copy(me - 1).wait_recv()

    prod[0:16, :] = rim_in[...]
    tap_rows = taps[:, pl.ds(my_lane, local_width)].astype(F32)
    conv_rows = 64

    def convolve(proj, dst, first):
        for i in range(own // conv_rows):
            row = pl.multiple_of(first + i * conv_rows, conv_rows)
            rows = slice(i * conv_rows, (i + 1) * conv_rows)
            window = prod[pl.ds(row, conv_rows + 16), :].astype(F32)
            mixed = window[14 : 14 + conv_rows] * tap_rows[0:1]
            mixed = mixed + window[15 : 15 + conv_rows] * tap_rows[1:2]
            mixed = mixed + window[16 : 16 + conv_rows] * tap_rows[2:3]
            dst[rows, :] = (proj[GO_][rows, :].astype(F32) * mixed).astype(BF16)

    convolve(proj_peer, conv_peer, peer_row)
    send_conv = pltpu.make_async_remote_copy(
        src_ref=conv_peer, dst_ref=conv_in, send_sem=conv_s, recv_sem=conv_r, **peer
    )
    project_sig(x_peer, sig_peer)
    send_conv.start()
    convolve(proj_own, conv_own, my_row)
    start_log = jnp.zeros((heads, BLOCK), F32)
    for i in range(n_sp - 1):
        merged = jnp.maximum(scal_in[i, 0:heads, :] + start_log, scal_in[i, heads : 2 * heads, :])
        start_log = jnp.where(i < me, merged, start_log)
    carried_log = table[T_CARRY] + jnp.concatenate([start_log] * nblocks, axis=0)
    new_top = jnp.maximum(table[T_TOP], carried_log)
    keep = jnp.exp(table[T_TOP] - new_top)
    bring = jnp.exp(carried_log - new_top)
    for b in range(nblocks):
        rows = slice(b * heads, (b + 1) * heads)
        cols_in[b] = jnp.concatenate([keep[rows], bring[rows], fill], axis=0).T
    acc[...] = jnp.dot(conv_own[...], woc[...], preferred_element_type=F32)

    def wait_state(k, carry):
        source = lax.rem(me + k, n_sp)
        pltpu.make_async_remote_copy(
            src_ref=state_out.at[source], dst_ref=state_in.at[source],
            send_sem=st_s.at[source], recv_sem=st_r.at[source], **sp(source),
        ).wait_recv()
        return carry

    lax.fori_loop(1, n_sp, wait_state, 0)
    send_conv.wait_recv()
    for copy in out_weights:
        copy.wait_recv()

    piece_blocks = piece_rows // BLOCK

    def bring_in(proj, piece):
        return [
            [
                jnp.dot(
                    proj[Q_][block * BLOCK : (block + 1) * BLOCK, h * dh : (h + 1) * dh],
                    state_in[h * per_head : (h + 1) * per_head].reshape(dh, dh),
                    preferred_element_type=F32,
                )
                for h in range(heads)
            ]
            for block in range(piece * piece_blocks, (piece + 1) * piece_blocks)
        ]

    def finish(brought, read, sig, dst, piece, first):
        for i in range(piece_blocks):
            block = piece * piece_blocks + i
            rows = slice(block * BLOCK, (block + 1) * BLOCK)
            columns = cols_in[first + block]
            for h in range(heads):
                hs = slice(h * dh, (h + 1) * dh)
                readout = (
                    columns[:, h : h + 1] * read[rows, hs]
                    + columns[:, heads + h : heads + h + 1] * brought[i][h]
                )
                normalized = readout * lax.rsqrt(
                    jnp.mean(readout * readout, axis=-1, keepdims=True) + EPSILON
                )
                dst[i * BLOCK : (i + 1) * BLOCK, hs] = (normalized * sig[rows, hs]).astype(BF16)

    def send_memory(i, mem):
        return pltpu.make_async_remote_copy(
            src_ref=mem, dst_ref=mem_in.at[i], send_sem=mem_s.at[i], recv_sem=mem_r.at[i], **peer
        )

    def add_part(at, rows, weight):
        acc[at, :] = acc[at, :] + jnp.dot(rows, weight[...], preferred_element_type=F32)

    brought_0 = bring_in(proj_peer, 0)
    brought_1 = bring_in(proj_peer, 1)
    finish(brought_0, read_peer, sig_peer, mem_0, 0, peer_block)
    send_memory(0, mem_0).start()
    add_part(spans[0], conv_in[spans[0], :], woc_in)
    finish(brought_1, read_peer, sig_peer, mem_1, 1, peer_block)
    send_memory(1, mem_1).start()
    brought_2 = bring_in(proj_own, 0)
    finish(brought_2, read_own, sig_own, mem_2, 0, my_block)
    add_part(spans[1], conv_in[spans[1], :], woc_in)
    brought_3 = bring_in(proj_own, 1)
    finish(brought_3, read_own, sig_own, mem_3, 1, my_block)
    add_part(spans[0], mem_2[...], wom)
    add_part(spans[1], mem_3[...], wom)

    for i, at in enumerate(spans):
        send_memory(i, (mem_0, mem_1)[i]).wait_recv()
    for i, at in enumerate(spans):
        out[0, at, :] = (
            acc[at, :] + jnp.dot(mem_in[i], wom_in[...], preferred_element_type=F32)
        ).astype(BF16)

    send_rows.wait_send()
    send_gates.wait_send()

    @pl.when(jnp.logical_not(last))
    def _():
        rim_copy(me + 1).wait_send()

    def drain(k, carry):
        target = lax.rem(me + k, n_sp)
        for copy in segment_copies(target):
            copy.wait_send()
        pltpu.make_async_remote_copy(
            src_ref=state_out.at[target], dst_ref=state_in.at[me],
            send_sem=st_s.at[target], recv_sem=st_r.at[me], **sp(target),
        ).wait_send()
        return carry

    lax.fori_loop(1, n_sp, drain, 0)
    send_conv.wait_send()
    for copy in out_weights:
        copy.wait_send()
    for i, mem in enumerate((mem_0, mem_1)):
        send_memory(i, mem).wait_send()


def store_kernel(src, dst, sems):
    rows = src.shape[1] // 4
    copies = [
        pltpu.make_async_copy(
            src.at[0, pl.ds(i * rows, rows), :], dst.at[0, pl.ds(i * rows, rows), :], sems.at[i]
        )
        for i in range(4)
    ]
    for copy in copies:
        copy.start()
    for copy in copies:
        copy.wait()


def local_layer(
    n_sp,
    tokens, norm_gain, w_query, w_key, w_value, w_outgate, w_gatein, w_gateout, w_convin,
    w_igate, w_fgate, input_bias, forget_bias, forget_extra, init_memory, head_gain, conv_taps,
    out_memory, out_conv,
):
    own, width = tokens.shape[1:]
    count = 2 * own
    local_width = w_query.shape[1]
    heads, dh = init_memory.shape[1], init_memory.shape[3]
    nblocks = count // BLOCK
    slice_rows = heads * dh // n_sp
    vmem = pltpu.VMEM
    dma = pltpu.SemaphoreType.DMA
    half = vmem((own, local_width), BF16)
    half_wide = vmem((own, local_width), F32)
    quarter = vmem((own // 2, local_width), BF16)
    scratch = [
        vmem((own, width), BF16),
        vmem((width // 128, 128), BF16),
        [vmem((width, local_width), BF16)] * 7,
        vmem((local_width, width), BF16),
        vmem((local_width, width), BF16),
        vmem((2 * heads, width), BF16),
        vmem((2 * heads, width), BF16),
        vmem((4 * heads, count), F32),
        vmem((heads, count), F32),
        vmem((1, 2 * heads), F32),
        vmem((1, 2 * heads), F32),
        vmem(conv_taps.shape, BF16),
        vmem((2 * heads, dh), BF16),
        vmem((slice_rows, dh), F32),
        vmem((own, width), BF16),
        vmem((own, width), BF16),
        [half] * 7,
        [half] * 7,
        half_wide, half_wide,
        half_wide, half_wide,
        half, half, half,
        vmem((own, width), F32),
        quarter, quarter, quarter, quarter,
        vmem((2, own // 2, local_width), BF16),
        vmem((local_width, width), BF16),
        vmem((local_width, width), BF16),
        vmem((nblocks, heads, dh, 2 * BLOCK), BF16),
        vmem((6, nblocks * heads, BLOCK), F32),
        vmem((nblocks, BLOCK, BLOCK), F32),
        vmem((nblocks, BLOCK, BLOCK), F32),
        vmem((nblocks, heads, dh, dh), F32),
        vmem((n_sp, slice_rows, dh), BF16),
        vmem((n_sp, slice_rows, dh), BF16),
        vmem((2 * heads, BLOCK), F32),
        vmem((n_sp, 2 * heads, BLOCK), F32),
        vmem((n_sp, slice_rows, dh), BF16),
        vmem((n_sp, slice_rows, dh), BF16),
        vmem((16, local_width), BF16),
        vmem((count + 16, local_width), BF16),
        pltpu.SemaphoreType.REGULAR,
        dma((L_W + 7,)),
        dma, dma, dma, dma,
        dma((n_sp,)), dma((n_sp,)),
        dma((n_sp,)), dma((n_sp,)),
        dma((n_sp,)), dma((n_sp,)),
        dma, dma,
        dma((2,)), dma((2,)),
        dma, dma,
        dma((2,)), dma((2,)),
    ]
    rows = pl.pallas_call(
        functools.partial(kernel, n_sp),
        out_shape=vmem(tokens.shape, BF16),
        in_specs=[pl.BlockSpec(memory_space=pl.ANY)] * 19,
        out_specs=pl.BlockSpec(memory_space=pltpu.VMEM),
        scratch_shapes=scratch,
        compiler_params=pltpu.CompilerParams(
            collective_id=0, has_side_effects=True, vmem_limit_bytes=58 * 1024 * 1024
        ),
    )(
        tokens, norm_gain.reshape(-1, 128),
        w_query, w_key, w_value, w_outgate, w_gatein, w_gateout, w_convin,
        w_igate.T, w_fgate.T, input_bias.reshape(1, -1), forget_bias.reshape(1, -1),
        jnp.swapaxes(forget_extra, 1, 2), init_memory, head_gain.reshape(-1, dh), conv_taps,
        out_memory, out_conv,
    )
    return pl.pallas_call(
        store_kernel,
        out_shape=jax.ShapeDtypeStruct(tokens.shape, BF16),
        in_specs=[pl.BlockSpec(memory_space=pltpu.VMEM)],
        out_specs=pl.BlockSpec(memory_space=pl.ANY),
        scratch_shapes=[dma((4,))],
    )(pltpu.with_memory_space_constraint(rows, pltpu.VMEM))


def solution(mesh):
    rows = P("fs", ("sp", "tp"), None)
    column, replicated = P(None, "tp"), P()
    return jax.shard_map(
        functools.partial(local_layer, mesh.shape["sp"]),
        mesh=mesh,
        in_specs=(
            rows, replicated,
            column, column, column, column, column, column, column,
            replicated, replicated, replicated, replicated,
            P("fs", "sp", "tp"), P("fs", "tp", None, None),
            replicated, replicated,
            P("tp", None), P("tp", None),
        ),
        out_specs=rows,
        check_vma=False,
    )
```

```python
import functools
import math

import jax
import jax.numpy as jnp
from jax import lax
from jax.experimental import pallas as pl
from jax.experimental.pallas import tpu as pltpu
from jax.sharding import PartitionSpec as P

MESH = pl.DeviceIdType.MESH
F32 = jnp.float32
BF16 = jnp.bfloat16
BLOCK = 128
EPSILON = 1e-06
LOWEST_LOG = -1e30

K_, V_, Q_, OG_, GI_, CI_, GO_ = range(7)
T_BIAS, T_KW, T_ALPHA, T_BETA, T_TOP, T_CARRY = range(6)
L_TOK, L_WIG, L_WFG, L_GAIN, L_FE, L_IB, L_FB, L_TAPS, L_HG, L_OM, L_OC, L_INIT, L_W = (
    0, 4, 5, 6, 7, 8, 9, 10, 11, 12, 13, 14, 16,
)


def kernel(
    n_sp,
    tokens, norm_gain, w_query, w_key, w_value, w_outgate, w_gatein, w_gateout, w_convin,
    w_igate, w_fgate, input_bias, forget_bias, forget_extra, init_memory, head_gain, conv_taps,
    out_memory, out_conv,
    acc, mem_in, wom_in,
    tok, gain, w_all, wom, woc, wig, wfg, gates, fe, ib, fb, taps, hg, init,
    x_own, x_peer, proj_own, proj_peer, sig_own, sig_peer, read_own, read_peer,
    conv_own, conv_peer, conv_in, mem_0, mem_1, mem_2, mem_3, woc_in,
    keys, table, cols, cols_in, terms, seg, seg_in, scal, scal_in, state_out, state_in,
    rim_in, prod,
    ready, lsem, tok_s, tok_r, gate_s, gate_r, seg_s, seg_r, scal_s, scal_r, st_s, st_r,
    rim_s, rim_r, ow_s, ow_r, conv_s, conv_r, mem_s, mem_r,
):
    own = tokens.shape[1]
    count = 2 * own
    local_width = w_query.shape[1]
    heads = init_memory.shape[1]
    dh = init_memory.shape[3]
    nblocks = count // BLOCK
    half_blocks = nblocks // 2
    slice_rows = heads * dh // n_sp
    per_head = dh // slice_rows
    key_log = -0.5 * math.log(dh)
    me = lax.axis_index("sp")
    side = lax.axis_index("tp")
    other = 1 - side
    my_row = pl.multiple_of(side * own, own)
    peer_row = pl.multiple_of(other * own, own)
    my_block = side * half_blocks
    peer_block = other * half_blocks
    my_head = (me * slice_rows) // dh
    my_depth = pl.multiple_of(me * slice_rows - my_head * dh, slice_rows)
    my_lane = pl.multiple_of(side * local_width, local_width)
    my_rows = pl.ds(my_row, own)
    peer_rows = pl.ds(peer_row, own)

    def local(src, dst, index):
        return pltpu.make_async_copy(src, dst, lsem.at[index])

    def sp(target):
        return dict(device_id={"sp": target}, device_id_type=MESH)

    peer = dict(device_id={"tp": other}, device_id_type=MESH)
    weights = (w_key, w_value, w_query, w_outgate, w_gatein, w_convin, w_gateout)

    barrier = pltpu.get_barrier_semaphore()
    chunks = 4
    chunk_rows = own // chunks
    token_copies = [
        local(
            tokens.at[0, pl.ds(c * chunk_rows, chunk_rows), :],
            tok.at[pl.ds(c * chunk_rows, chunk_rows), :],
            L_TOK + c,
        )
        for c in range(chunks)
    ]
    gain_copy = local(norm_gain, gain, L_GAIN)
    narrow_copies = [local(w_igate, wig, L_WIG), local(w_fgate, wfg, L_WFG)]
    w_copies = [local(weights[p], w_all[p], L_W + p) for p in range(7)]
    gate_copies = [
        local(forget_extra.at[0], fe, L_FE),
        local(input_bias, ib, L_IB),
        local(forget_bias, fb, L_FB),
    ]
    head_copy = local(head_gain, hg, L_HG)
    taps_copy = local(conv_taps, taps, L_TAPS)
    init_copy = local(init_memory.at[0, my_head, pl.ds(my_depth, slice_rows), :], init, L_INIT)
    out_copies = [local(out_conv, woc, L_OC), local(out_memory, wom, L_OM)]
    gain_copy.start()
    for copy in token_copies + narrow_copies + w_copies[:2] + gate_copies:
        copy.start()
    pl.semaphore_signal(barrier, inc=1, **peer)

    def greet(k, carry):
        pl.semaphore_signal(barrier, inc=1, **sp(k))
        return carry

    lax.fori_loop(me + 1, n_sp, greet, 0)

    gain_copy.wait()
    gain_row = jnp.concatenate(
        [gain[i : i + 1, :] for i in range(gain.shape[0])], axis=1
    ).astype(F32)
    norm_rows = 16

    def own_gates(c):
        rows = x_own[c * chunk_rows : (c + 1) * chunk_rows, :]
        gates[:, pl.ds(my_row + c * chunk_rows, chunk_rows)] = lax.dot_general(
            narrow, rows, (((1,), (1,)), ((), ())), preferred_element_type=F32
        )

    for c in range(chunks):
        token_copies[c].wait()
        if c == 1:
            for copy in narrow_copies:
                copy.wait()
            narrow = jnp.concatenate([wig[...], wfg[...]], axis=0)
        if c > 0:
            own_gates(c - 1)
        for start in range(c * chunk_rows, (c + 1) * chunk_rows, norm_rows):
            rows = slice(start, start + norm_rows)
            values = tok[rows, :].astype(F32)
            scale = lax.rsqrt(jnp.mean(values * values, axis=-1, keepdims=True) + EPSILON)
            x_own[rows, :] = (values * scale * gain_row).astype(BF16)
    own_gates(chunks - 1)

    pl.semaphore_wait(barrier, me + 1)
    send_rows = pltpu.make_async_remote_copy(
        src_ref=x_own, dst_ref=x_peer, send_sem=tok_s, recv_sem=tok_r, **peer
    )
    send_gates = pltpu.make_async_remote_copy(
        src_ref=gates.at[:, my_rows], dst_ref=gates.at[:, my_rows],
        send_sem=gate_s, recv_sem=gate_r, **peer,
    )
    take_gates = pltpu.make_async_remote_copy(
        src_ref=gates.at[:, peer_rows], dst_ref=gates.at[:, peer_rows],
        send_sem=gate_s, recv_sem=gate_r, **peer,
    )
    send_gates.start()
    send_rows.start()

    def answer(k, carry):
        pl.semaphore_signal(ready, inc=1, **sp(k))
        return carry

    lax.fori_loop(0, me, answer, 0)

    pieces = 2
    piece_rows = own // pieces
    spans = [slice(i * piece_rows, (i + 1) * piece_rows) for i in range(pieces)]

    def project(p, rows, dst):
        for at in spans:
            dst[p][at, :] = jnp.dot(
                rows[at, :], w_all[p][...], preferred_element_type=F32
            ).astype(BF16)

    def head_gains():
        gains = hg[...].astype(F32)
        gains = jnp.where(side == 0, gains[0:heads], gains[heads : 2 * heads])
        return jnp.concatenate([gains[i : i + 1] for i in range(heads)], axis=1)

    def sig_piece(rows, dst, i):
        at = spans[i]
        value = jnp.dot(rows[at, :], w_all[OG_][...], preferred_element_type=F32).astype(BF16)
        dst[at, :] = head_gains() * jax.nn.sigmoid(value.astype(F32))

    def piece_of(p, rows, dst, i):
        at = spans[i]
        dst[p][at, :] = jnp.dot(
            rows[at, :], w_all[p][...], preferred_element_type=F32
        ).astype(BF16)

    def prod_piece(rows, proj, row, i):
        at = spans[i]
        value = jnp.dot(rows[at, :], w_all[CI_][...], preferred_element_type=F32).astype(BF16)
        prod[pl.ds(row + 16 + i * piece_rows, piece_rows), :] = (
            proj[GI_][at, :].astype(F32) * value.astype(F32)
        ).astype(BF16)

    w_copies[K_].wait()
    w_copies[V_].wait()
    for copy in w_copies[2:4] + [head_copy] + w_copies[4:]:
        copy.start()
    for copy in [taps_copy, init_copy] + out_copies:
        copy.start()
    project(K_, x_own, proj_own)
    project(V_, x_own, proj_own)
    w_copies[Q_].wait()
    w_copies[OG_].wait()
    head_copy.wait()
    for copy in gate_copies:
        copy.wait()
    take_gates.wait_recv()

    lanes = lax.broadcasted_iota(jnp.int32, (nblocks * heads, BLOCK), 1)
    head_rows = lax.broadcasted_iota(jnp.int32, (heads, BLOCK), 0)
    bias_in = jnp.zeros((heads, BLOCK), F32)
    bias_forget = jnp.zeros((heads, BLOCK), F32)
    for h in range(heads):
        for part_index in range(2):
            pick = (head_rows == h) & (side == part_index)
            c = part_index * heads + h
            bias_in = jnp.where(pick, ib[0:1, c : c + 1], bias_in)
            bias_forget = jnp.where(pick, fb[0:1, c : c + 1], bias_forget)
    ins, forgets = [], []
    for b in range(nblocks):
        at = slice(b * BLOCK, (b + 1) * BLOCK)
        pre = gates[:, at]
        ins.append(jnp.where(side == 0, pre[0:heads], pre[heads : 2 * heads]) + bias_in)
        forget = (
            jnp.where(side == 0, pre[2 * heads : 3 * heads], pre[3 * heads : 4 * heads])
            + bias_forget
        )
        forgets.append(
            jnp.minimum(forget, 0.0) - jnp.log1p(jnp.exp(-jnp.abs(forget))) + fe[:, at]
        )
    ins = jnp.concatenate(ins, axis=0)
    cumulative = jnp.concatenate(forgets, axis=0)
    shift = 1
    while shift < BLOCK:
        cumulative = cumulative + jnp.where(
            lanes >= shift, pltpu.roll(cumulative, shift, 1), 0.0
        )
        shift *= 2
    pair = ins - cumulative
    top = pair
    shift = 1
    while shift < BLOCK:
        top = jnp.maximum(top, jnp.where(lanes >= shift, pltpu.roll(top, shift, 1), top))
        shift *= 2
    total = jnp.broadcast_to(cumulative[:, BLOCK - 1 :], cumulative.shape)
    last_top = jnp.broadcast_to(top[:, BLOCK - 1 :], top.shape)
    log_scale = jnp.full((heads, BLOCK), LOWEST_LOG, F32)
    before = jnp.zeros((heads, BLOCK), F32)
    scales, befores, alphas, betas = [], [], [], []
    for b in range(nblocks):
        block_total = total[b * heads : (b + 1) * heads]
        block_top = block_total + last_top[b * heads : (b + 1) * heads]
        scales.append(log_scale)
        befores.append(before)
        merged = jnp.maximum(block_total + log_scale, block_top)
        alphas.append(block_total + log_scale - merged)
        betas.append(block_top - merged)
        log_scale = merged
        before = before + block_total
    scal[0:heads, :] = before
    scal[heads : 2 * heads, :] = log_scale
    scal_in[me] = scal[...]
    scales = jnp.concatenate(scales, axis=0)
    row_top = jnp.maximum(scales, top)
    table[T_BIAS] = pair + key_log
    table[T_KW] = jnp.exp(pair + key_log - last_top)
    table[T_ALPHA] = jnp.exp(jnp.concatenate(alphas, axis=0))
    table[T_BETA] = jnp.exp(jnp.concatenate(betas, axis=0))
    table[T_TOP] = row_top
    table[T_CARRY] = jnp.concatenate(befores, axis=0)
    carry_weight = jnp.exp(scales - row_top)
    fill = jnp.zeros((BLOCK - 2 * heads, BLOCK), F32)
    for b in range(nblocks):
        rows = slice(b * heads, (b + 1) * heads)
        cols[b] = jnp.concatenate([row_top[rows], carry_weight[rows], fill], axis=0).T
    project(Q_, x_own, proj_own)
    sig_piece(x_own, sig_own, 0)
    sig_piece(x_own, sig_own, 1)

    def weigh_keys(proj, first):
        weighted = []
        for i in range(half_blocks):
            rows = slice(i * BLOCK, (i + 1) * BLOCK)
            b = first + i
            for h in range(heads):
                turned = proj[K_][rows, h * dh : (h + 1) * dh].T
                keys[b, h, :, 0:BLOCK] = turned
                weighted.append(
                    (turned.astype(F32) * table[T_KW, pl.ds(b * heads + h, 1), :]).astype(BF16)
                )
        return weighted

    def block_terms(weighted, proj, first):
        for i in range(half_blocks):
            rows = slice(i * BLOCK, (i + 1) * BLOCK)
            for h in range(heads):
                terms[first + i, h] = jnp.dot(
                    weighted[i * heads + h], proj[V_][rows, h * dh : (h + 1) * dh],
                    preferred_element_type=F32,
                )

    w_copies[GI_].wait()
    w_copies[CI_].wait()
    w_copies[GO_].wait()
    take_rows = pltpu.make_async_remote_copy(
        src_ref=x_own, dst_ref=x_peer, send_sem=tok_s, recv_sem=tok_r, **peer
    )
    take_rows.wait_recv()
    out_weights = [
        pltpu.make_async_remote_copy(
            src_ref=src, dst_ref=dst, send_sem=ow_s.at[i], recv_sem=ow_r.at[i], **peer
        )
        for i, (src, dst) in enumerate(((out_conv, woc_in), (out_memory, wom_in)))
    ]
    for copy in out_weights:
        copy.start()
    weighted_own = weigh_keys(proj_own, my_block)
    project(K_, x_peer, proj_peer)
    block_terms(weighted_own, proj_own, my_block)
    weighted_peer = weigh_keys(proj_peer, peer_block)
    project(V_, x_peer, proj_peer)
    block_terms(weighted_peer, proj_peer, peer_block)

    @pl.when(me < n_sp - 1)
    def _():
        pl.semaphore_wait(ready, n_sp - 1 - me)

    piece_of(GI_, x_own, proj_own, 0)
    for h in range(heads):
        held = jnp.zeros((dh, dh), F32)
        for b in range(nblocks):
            at = pl.ds(b * heads + h, 1)
            keys[b, h, :, BLOCK:] = held.astype(BF16)
            held = table[T_ALPHA, at, :] * held + table[T_BETA, at, :] * terms[b, h]
        for piece in range(per_head):
            seg[h * per_head + piece] = held[
                piece * slice_rows : (piece + 1) * slice_rows, :
            ].astype(BF16)
    seg_in[me] = seg[me]

    def segment_copies(target):
        return (
            pltpu.make_async_remote_copy(
                src_ref=scal, dst_ref=scal_in.at[me],
                send_sem=scal_s.at[target], recv_sem=scal_r.at[me], **sp(target),
            ),
            pltpu.make_async_remote_copy(
                src_ref=seg.at[target], dst_ref=seg_in.at[me],
                send_sem=seg_s.at[target], recv_sem=seg_r.at[me], **sp(target),
            ),
        )

    for k in range(1, n_sp):
        for copy in segment_copies(lax.rem(me + k, n_sp)):
            copy.start()
    piece_of(GI_, x_own, proj_own, 1)

    t_index = lax.broadcasted_iota(jnp.int32, (BLOCK, BLOCK), 0)
    s_index = lax.broadcasted_iota(jnp.int32, (BLOCK, BLOCK), 1)
    causal = s_index <= t_index

    def read_blocks(proj, read, first, chunks, middle=None):
        def scores_of(i):
            rows = slice(i * BLOCK, (i + 1) * BLOCK)
            return [
                jnp.dot(
                    proj[Q_][rows, h * dh : (h + 1) * dh], keys[first + i, h],
                    preferred_element_type=F32,
                )
                for h in range(heads)
            ]

        def weigh(i, raw):
            columns = cols[first + i]
            weighted, carried = [], []
            for h in range(heads):
                log_weight = jnp.where(
                    causal,
                    table[T_BIAS, pl.ds((first + i) * heads + h, 1), :] - columns[:, h : h + 1],
                    -jnp.inf,
                )
                weighted.append((jnp.exp(log_weight) * raw[h][:, 0:BLOCK]).astype(BF16))
                carried.append(columns[:, heads + h : heads + h + 1] * raw[h][:, BLOCK:])
            return weighted, carried

        def read_out(i, weighted, carried):
            rows = slice(i * BLOCK, (i + 1) * BLOCK)
            for h in range(heads):
                hs = slice(h * dh, (h + 1) * dh)
                read[rows, hs] = carried[h] + jnp.dot(
                    weighted[h], proj[V_][rows, hs], preferred_element_type=F32
                )

        raw = scores_of(0)
        for i in range(half_blocks):
            parts = weigh(i, raw)
            chunks[i]()
            if i + 1 < half_blocks:
                raw = scores_of(i + 1)
            read_out(i, *parts)
            if middle is not None and i + 1 == half_blocks // 2:
                middle()
        for chunk in chunks[half_blocks:]:
            chunk()

    read_blocks(
        proj_own, read_own, my_block,
        [
            lambda: prod_piece(x_own, proj_own, my_row, 0),
            lambda: prod_piece(x_own, proj_own, my_row, 1),
            lambda: piece_of(GI_, x_peer, proj_peer, 0),
            lambda: piece_of(GI_, x_peer, proj_peer, 1),
        ],
    )
    project(Q_, x_peer, proj_peer)

    def owner_step():
        init_copy.wait()

        def wait_segment(k, carry):
            source = lax.rem(me + k, n_sp)
            pltpu.make_async_remote_copy(
                src_ref=scal, dst_ref=scal_in.at[source],
                send_sem=scal_s.at[source], recv_sem=scal_r.at[source], **sp(source),
            ).wait_recv()
            pltpu.make_async_remote_copy(
                src_ref=seg.at[source], dst_ref=seg_in.at[source],
                send_sem=seg_s.at[source], recv_sem=seg_r.at[source], **sp(source),
            ).wait_recv()
            return carry

        lax.fori_loop(1, n_sp, wait_segment, 0)
        state = init[...]
        state_log = jnp.zeros((1, BLOCK), F32)
        for i in range(n_sp):
            state_out[i] = state.astype(BF16)
            if i == n_sp - 1:
                break
            span = scal_in[i, pl.ds(my_head, 1), :]
            span_top = scal_in[i, pl.ds(heads + my_head, 1), :]
            merged = jnp.maximum(span + state_log, span_top)
            state = (
                jnp.exp(span + state_log - merged) * state
                + jnp.exp(span_top - merged) * seg_in[i].astype(F32)
            )
            state_log = merged
        state_in[me] = state_out[me]

        def send_state(k, carry):
            target = lax.rem(me + k, n_sp)
            pltpu.make_async_remote_copy(
                src_ref=state_out.at[target], dst_ref=state_in.at[me],
                send_sem=st_s.at[target], recv_sem=st_r.at[me], **sp(target),
            ).start()
            return carry

        lax.fori_loop(1, n_sp, send_state, 0)

    along_x, along_z = lax.rem(me, 4), me // 4
    lateness = 2 * along_z + jnp.where(along_x == 3, 3, 2 * along_x)
    late = lateness >= 7
    between = (lateness >= 4) & (lateness < 7)
    soon = (lateness >= 1) & (lateness < 4)
    first = lateness < 1
    pl.when(late)(owner_step)

    prod_piece(x_peer, proj_peer, peer_row, 0)
    prod_piece(x_peer, proj_peer, peer_row, 1)

    def rim_copy(target):
        return pltpu.make_async_remote_copy(
            src_ref=prod.at[pl.ds(count, 16), :], dst_ref=rim_in,
            send_sem=rim_s, recv_sem=rim_r, **sp(target),
        )

    last = me == n_sp - 1

    @pl.when(jnp.logical_not(last))
    def _():
        rim_copy(me + 1).start()

    pl.when(between)(owner_step)

    read_blocks(
        proj_peer, read_peer, peer_block,
        [
            lambda: piece_of(GO_, x_peer, proj_peer, 0),
            lambda: piece_of(GO_, x_peer, proj_peer, 1),
            lambda: piece_of(GO_, x_own, proj_own, 0),
            lambda: piece_of(GO_, x_own, proj_own, 1),
        ],
        middle=lambda: pl.when(soon)(owner_step),
    )

    pl.when(first)(owner_step)

    taps_copy.wait()
    for copy in out_copies:
        copy.wait()
    tap_rows = taps[:, pl.ds(my_lane, local_width)].astype(F32)
    conv_rows = 64

    def convolve(proj, dst, first, part):
        for i in part:
            row = pl.multiple_of(first + i * conv_rows, conv_rows)
            rows = slice(i * conv_rows, (i + 1) * conv_rows)
            window = prod[pl.ds(row, conv_rows + 16), :].astype(F32)
            mixed = window[14 : 14 + conv_rows] * tap_rows[0:1]
            mixed = mixed + window[15 : 15 + conv_rows] * tap_rows[1:2]
            mixed = mixed + window[16 : 16 + conv_rows] * tap_rows[2:3]
            dst[rows, :] = (proj[GO_][rows, :].astype(F32) * mixed).astype(BF16)

    conv_steps = range(own // conv_rows)

    def send_conv(i):
        at = (pl.ds(conv_rows, own - conv_rows), pl.ds(0, conv_rows))[i]
        return pltpu.make_async_remote_copy(
            src_ref=conv_peer.at[at, :], dst_ref=conv_in.at[at, :],
            send_sem=conv_s.at[i], recv_sem=conv_r.at[i], **peer,
        )

    sig_piece(x_peer, sig_peer, 0)
    convolve(proj_peer, conv_peer, peer_row, conv_steps[1:])
    send_conv(0).start()
    sig_piece(x_peer, sig_peer, 1)
    convolve(proj_own, conv_own, my_row, conv_steps[1:])
    start_log = jnp.zeros((heads, BLOCK), F32)
    for i in range(n_sp - 1):
        merged = jnp.maximum(scal_in[i, 0:heads, :] + start_log, scal_in[i, heads : 2 * heads, :])
        start_log = jnp.where(i < me, merged, start_log)
    carried_log = table[T_CARRY] + jnp.concatenate([start_log] * nblocks, axis=0)
    new_top = jnp.maximum(table[T_TOP], carried_log)
    keep = jnp.exp(table[T_TOP] - new_top)
    bring = jnp.exp(carried_log - new_top)
    for b in range(nblocks):
        rows = slice(b * heads, (b + 1) * heads)
        cols_in[b] = jnp.concatenate([keep[rows], bring[rows], fill], axis=0).T

    @pl.when(me == 0)
    def _():
        rim_in[...] = jnp.zeros_like(rim_in)

    @pl.when(me > 0)
    def _():
        rim_copy(me - 1).wait_recv()

    prod[0:16, :] = rim_in[...]
    convolve(proj_peer, conv_peer, peer_row, conv_steps[:1])
    convolve(proj_own, conv_own, my_row, conv_steps[:1])
    send_conv(1).start()

    def scale_parts(proj, read, first):
        for block in range(half_blocks):
            rows = slice(block * BLOCK, (block + 1) * BLOCK)
            columns = cols_in[first + block]
            for h in range(heads):
                hs = slice(h * dh, (h + 1) * dh)
                read[rows, hs] = columns[:, h : h + 1] * read[rows, hs]
                proj[Q_][rows, hs] = (
                    columns[:, heads + h : heads + h + 1] * proj[Q_][rows, hs].astype(F32)
                ).astype(BF16)

    column = acc.shape[1] // 4
    for j in range(4):
        at = slice(j * column, (j + 1) * column)
        acc[:, at] = jnp.dot(conv_own[...], woc[:, at], preferred_element_type=F32)
        if j == 0:
            scale_parts(proj_peer, read_peer, peer_block)
        if j == 2:
            scale_parts(proj_own, read_own, my_block)

    def wait_state(k, carry):
        source = lax.rem(me + k, n_sp)
        pltpu.make_async_remote_copy(
            src_ref=state_out.at[source], dst_ref=state_in.at[source],
            send_sem=st_s.at[source], recv_sem=st_r.at[source], **sp(source),
        ).wait_recv()
        return carry

    lax.fori_loop(1, n_sp, wait_state, 0)
    for i in range(2):
        send_conv(i).wait_recv()
    for copy in out_weights:
        copy.wait_recv()

    piece_blocks = piece_rows // BLOCK

    def bring_in(proj, piece):
        return [
            [
                jnp.dot(
                    proj[Q_][block * BLOCK : (block + 1) * BLOCK, h * dh : (h + 1) * dh],
                    state_in[h * per_head : (h + 1) * per_head].reshape(dh, dh),
                    preferred_element_type=F32,
                )
                for h in range(heads)
            ]
            for block in range(piece * piece_blocks, (piece + 1) * piece_blocks)
        ]

    def finish(brought, read, sig, dst, piece):
        for i in range(piece_blocks):
            block = piece * piece_blocks + i
            rows = slice(block * BLOCK, (block + 1) * BLOCK)
            for h in range(heads):
                hs = slice(h * dh, (h + 1) * dh)
                readout = read[rows, hs] + brought[i][h]
                normalized = readout * lax.rsqrt(
                    jnp.mean(readout * readout, axis=-1, keepdims=True) + EPSILON
                )
                dst[i * BLOCK : (i + 1) * BLOCK, hs] = (normalized * sig[rows, hs]).astype(BF16)

    def send_memory(i, mem):
        return pltpu.make_async_remote_copy(
            src_ref=mem, dst_ref=mem_in.at[i], send_sem=mem_s.at[i], recv_sem=mem_r.at[i], **peer
        )

    def conv_part(j):
        at = slice(j * column, (j + 1) * column)
        acc[:, at] = acc[:, at] + jnp.dot(
            conv_in[...], woc_in[:, at], preferred_element_type=F32
        )

    def own_part(i, mem):
        acc[spans[i], :] = acc[spans[i], :] + jnp.dot(
            mem[...], wom[...], preferred_element_type=F32
        )

    brought_0 = bring_in(proj_peer, 0)
    conv_part(0)
    brought_1 = bring_in(proj_peer, 1)
    finish(brought_0, read_peer, sig_peer, mem_0, 0)
    send_memory(0, mem_0).start()
    conv_part(1)
    brought_2 = bring_in(proj_own, 0)
    finish(brought_1, read_peer, sig_peer, mem_1, 1)
    send_memory(1, mem_1).start()
    conv_part(2)
    brought_3 = bring_in(proj_own, 1)
    finish(brought_2, read_own, sig_own, mem_2, 0)
    conv_part(3)
    finish(brought_3, read_own, sig_own, mem_3, 1)
    own_part(0, mem_2)
    own_part(1, mem_3)

    for i in range(pieces):
        send_memory(i, (mem_0, mem_1)[i]).wait_recv()

    send_rows.wait_send()
    send_gates.wait_send()

    @pl.when(jnp.logical_not(last))
    def _():
        rim_copy(me + 1).wait_send()

    def drain(k, carry):
        target = lax.rem(me + k, n_sp)
        for copy in segment_copies(target):
            copy.wait_send()
        pltpu.make_async_remote_copy(
            src_ref=state_out.at[target], dst_ref=state_in.at[me],
            send_sem=st_s.at[target], recv_sem=st_r.at[me], **sp(target),
        ).wait_send()
        return carry

    lax.fori_loop(1, n_sp, drain, 0)
    for i in range(2):
        send_conv(i).wait_send()
    for copy in out_weights:
        copy.wait_send()
    for i, mem in enumerate((mem_0, mem_1)):
        send_memory(i, mem).wait_send()


def last_kernel(acc, mem_in, wom_in, out, stage, sems):
    rows = acc.shape[0] // 4
    copies = []
    for i in range(4):
        at = slice(i * rows, (i + 1) * rows)
        stage[at, :] = (
            acc[at, :]
            + jnp.dot(
                mem_in[i // 2, (i % 2) * rows : (i % 2 + 1) * rows, :], wom_in[...],
                preferred_element_type=F32,
            )
        ).astype(BF16)
        copy = pltpu.make_async_copy(
            stage.at[pl.ds(i * rows, rows), :], out.at[0, pl.ds(i * rows, rows), :], sems.at[i]
        )
        copy.start()
        copies.append(copy)
    for copy in copies:
        copy.wait()


def local_layer(
    n_sp,
    tokens, norm_gain, w_query, w_key, w_value, w_outgate, w_gatein, w_gateout, w_convin,
    w_igate, w_fgate, input_bias, forget_bias, forget_extra, init_memory, head_gain, conv_taps,
    out_memory, out_conv,
):
    own, width = tokens.shape[1:]
    count = 2 * own
    local_width = w_query.shape[1]
    heads, dh = init_memory.shape[1], init_memory.shape[3]
    nblocks = count // BLOCK
    slice_rows = heads * dh // n_sp
    vmem = pltpu.VMEM
    dma = pltpu.SemaphoreType.DMA
    half = vmem((own, local_width), BF16)
    half_wide = vmem((own, local_width), F32)
    quarter = vmem((own // 2, local_width), BF16)
    scratch = [
        vmem((own, width), BF16),
        vmem((width // 128, 128), BF16),
        [vmem((width, local_width), BF16)] * 7,
        vmem((local_width, width), BF16),
        vmem((local_width, width), BF16),
        vmem((2 * heads, width), BF16),
        vmem((2 * heads, width), BF16),
        vmem((4 * heads, count), F32),
        vmem((heads, count), F32),
        vmem((1, 2 * heads), F32),
        vmem((1, 2 * heads), F32),
        vmem(conv_taps.shape, BF16),
        vmem((2 * heads, dh), BF16),
        vmem((slice_rows, dh), F32),
        vmem((own, width), BF16),
        vmem((own, width), BF16),
        [half] * 7,
        [half] * 7,
        half_wide, half_wide,
        half_wide, half_wide,
        half, half, half,
        quarter, quarter, quarter, quarter,
        vmem((local_width, width), BF16),
        vmem((nblocks, heads, dh, 2 * BLOCK), BF16),
        vmem((6, nblocks * heads, BLOCK), F32),
        vmem((nblocks, BLOCK, BLOCK), F32),
        vmem((nblocks, BLOCK, BLOCK), F32),
        vmem((nblocks, heads, dh, dh), F32),
        vmem((n_sp, slice_rows, dh), BF16),
        vmem((n_sp, slice_rows, dh), BF16),
        vmem((2 * heads, BLOCK), F32),
        vmem((n_sp, 2 * heads, BLOCK), F32),
        vmem((n_sp, slice_rows, dh), BF16),
        vmem((n_sp, slice_rows, dh), BF16),
        vmem((16, local_width), BF16),
        vmem((count + 16, local_width), BF16),
        pltpu.SemaphoreType.REGULAR,
        dma((L_W + 7,)),
        dma, dma, dma, dma,
        dma((n_sp,)), dma((n_sp,)),
        dma((n_sp,)), dma((n_sp,)),
        dma((n_sp,)), dma((n_sp,)),
        dma, dma,
        dma((2,)), dma((2,)),
        dma((2,)), dma((2,)),
        dma((2,)), dma((2,)),
    ]
    acc, mem_in, wom_in = pl.pallas_call(
        functools.partial(kernel, n_sp),
        out_shape=(
            vmem((own, width), F32),
            vmem((2, own // 2, local_width), BF16),
            vmem((local_width, width), BF16),
        ),
        in_specs=[pl.BlockSpec(memory_space=pl.ANY)] * 19,
        out_specs=(pl.BlockSpec(memory_space=pltpu.VMEM),) * 3,
        scratch_shapes=scratch,
        compiler_params=pltpu.CompilerParams(
            collective_id=0, has_side_effects=True, vmem_limit_bytes=54 * 1024 * 1024
        ),
    )(
        tokens, norm_gain.reshape(-1, 128),
        w_query, w_key, w_value, w_outgate, w_gatein, w_gateout, w_convin,
        w_igate.T, w_fgate.T, input_bias.reshape(1, -1), forget_bias.reshape(1, -1),
        jnp.swapaxes(forget_extra, 1, 2), init_memory, head_gain.reshape(-1, dh), conv_taps,
        out_memory, out_conv,
    )
    return pl.pallas_call(
        last_kernel,
        out_shape=jax.ShapeDtypeStruct(tokens.shape, BF16),
        in_specs=[pl.BlockSpec(memory_space=pltpu.VMEM)] * 3,
        out_specs=pl.BlockSpec(memory_space=pl.ANY),
        scratch_shapes=[vmem((own, width), BF16), dma((4,))],
        compiler_params=pltpu.CompilerParams(vmem_limit_bytes=16 * 1024 * 1024),
    )(*(pltpu.with_memory_space_constraint(part, pltpu.VMEM) for part in (acc, mem_in, wom_in)))


def solution(mesh):
    rows = P("fs", ("sp", "tp"), None)
    column, replicated = P(None, "tp"), P()
    return jax.shard_map(
        functools.partial(local_layer, mesh.shape["sp"]),
        mesh=mesh,
        in_specs=(
            rows, replicated,
            column, column, column, column, column, column, column,
            replicated, replicated, replicated, replicated,
            P("fs", "sp", "tp"), P("fs", "tp", None, None),
            replicated, replicated,
            P("tp", None), P("tp", None),
        ),
        out_specs=rows,
        check_vma=False,
    )
```

```python
import functools
import math

import jax
import jax.numpy as jnp
from jax import lax
from jax.experimental import pallas as pl
from jax.experimental.pallas import tpu as pltpu
from jax.sharding import PartitionSpec as P

MESH = pl.DeviceIdType.MESH
F32 = jnp.float32
BF16 = jnp.bfloat16
BLOCK = 128
EPSILON = 1e-06
LOWEST_LOG = -1e30

K_, V_, Q_, OG_, GI_, CI_, GO_ = range(7)
T_BIAS, T_KW, T_ALPHA, T_BETA, T_TOP, T_CARRY = range(6)
L_TOK, L_WIG, L_WFG, L_GAIN, L_FE, L_IB, L_FB, L_TAPS, L_HG, L_OM, L_OC, L_INIT, L_W = (
    0, 4, 5, 6, 7, 8, 9, 10, 11, 12, 13, 14, 16,
)


def kernel(
    n_sp,
    tokens, norm_gain, w_query, w_key, w_value, w_outgate, w_gatein, w_gateout, w_convin,
    w_igate, w_fgate, input_bias, forget_bias, forget_extra, init_memory, head_gain, conv_taps,
    out_memory, out_conv,
    acc, mem_in, wom_in,
    tok, gain, w_all, wom, woc, wig, wfg, gates, fe, ib, fb, taps, hg, init,
    x_own, x_peer, proj_own, proj_peer, sig_own, sig_peer, read_own, read_peer,
    conv_own, conv_peer, conv_in, mem_0, mem_1, mem_2, mem_3, woc_in,
    keys, table, cols, cols_in, terms, seg, seg_in, scal, scal_in, state_out, state_in,
    rim_in, rim_out, prod_own, prod_peer,
    ready, lsem, tok_s, tok_r, gate_s, gate_r, seg_s, seg_r, scal_s, scal_r, st_s, st_r,
    rim_s, rim_r, ow_s, ow_r, conv_s, conv_r, mem_s, mem_r,
):
    own = tokens.shape[1]
    count = 2 * own
    local_width = w_query.shape[1]
    heads = init_memory.shape[1]
    dh = init_memory.shape[3]
    nblocks = count // BLOCK
    half_blocks = nblocks // 2
    slice_rows = heads * dh // n_sp
    per_head = dh // slice_rows
    key_log = -0.5 * math.log(dh)
    me = lax.axis_index("sp")
    side = lax.axis_index("tp")
    other = 1 - side
    my_row = pl.multiple_of(side * own, own)
    peer_row = pl.multiple_of(other * own, own)
    my_block = side * half_blocks
    peer_block = other * half_blocks
    my_head = (me * slice_rows) // dh
    my_depth = pl.multiple_of(me * slice_rows - my_head * dh, slice_rows)
    my_lane = pl.multiple_of(side * local_width, local_width)
    my_rows = pl.ds(my_row, own)
    peer_rows = pl.ds(peer_row, own)

    def local(src, dst, index):
        return pltpu.make_async_copy(src, dst, lsem.at[index])

    def sp(target):
        return dict(device_id={"sp": target}, device_id_type=MESH)

    peer = dict(device_id={"tp": other}, device_id_type=MESH)
    weights = (w_key, w_value, w_query, w_outgate, w_gatein, w_convin, w_gateout)

    barrier = pltpu.get_barrier_semaphore()
    chunks = 4
    chunk_rows = own // chunks
    token_copies = [
        local(
            tokens.at[0, pl.ds(c * chunk_rows, chunk_rows), :],
            tok.at[pl.ds(c * chunk_rows, chunk_rows), :],
            L_TOK + c,
        )
        for c in range(chunks)
    ]
    gain_copy = local(norm_gain, gain, L_GAIN)
    narrow_copies = [local(w_igate, wig, L_WIG), local(w_fgate, wfg, L_WFG)]
    w_copies = [local(weights[p], w_all[p], L_W + p) for p in range(7)]
    gate_copies = [
        local(forget_extra.at[0], fe, L_FE),
        local(input_bias, ib, L_IB),
        local(forget_bias, fb, L_FB),
    ]
    head_copy = local(head_gain, hg, L_HG)
    taps_copy = local(conv_taps, taps, L_TAPS)
    init_copy = local(init_memory.at[0, my_head, pl.ds(my_depth, slice_rows), :], init, L_INIT)
    out_copies = [local(out_conv, woc, L_OC), local(out_memory, wom, L_OM)]
    gain_copy.start()
    for copy in token_copies + narrow_copies + w_copies[:2] + gate_copies:
        copy.start()
    pl.semaphore_signal(barrier, inc=1, **peer)

    def greet(k, carry):
        pl.semaphore_signal(barrier, inc=1, **sp(k))
        return carry

    lax.fori_loop(me + 1, n_sp, greet, 0)

    gain_copy.wait()
    gain_row = jnp.concatenate(
        [gain[i : i + 1, :] for i in range(gain.shape[0])], axis=1
    ).astype(F32)
    norm_rows = 8

    def own_gates(c):
        rows = x_own[c * chunk_rows : (c + 1) * chunk_rows, :]
        gates[:, pl.ds(my_row + c * chunk_rows, chunk_rows)] = lax.dot_general(
            narrow, rows, (((1,), (1,)), ((), ())), preferred_element_type=F32
        )

    for c in range(chunks):
        token_copies[c].wait()
        if c == 1:
            for copy in narrow_copies:
                copy.wait()
            narrow = jnp.concatenate([wig[...], wfg[...]], axis=0)
        if c > 0:
            own_gates(c - 1)
        for start in range(c * chunk_rows, (c + 1) * chunk_rows, norm_rows):
            rows = slice(start, start + norm_rows)
            values = tok[rows, :].astype(F32)
            scale = lax.rsqrt(jnp.mean(values * values, axis=-1, keepdims=True) + EPSILON)
            x_own[rows, :] = (values * scale * gain_row).astype(BF16)
    own_gates(chunks - 1)

    pl.semaphore_wait(barrier, me + 1)
    send_rows = pltpu.make_async_remote_copy(
        src_ref=x_own, dst_ref=x_peer, send_sem=tok_s, recv_sem=tok_r, **peer
    )
    send_gates = pltpu.make_async_remote_copy(
        src_ref=gates.at[:, my_rows], dst_ref=gates.at[:, my_rows],
        send_sem=gate_s, recv_sem=gate_r, **peer,
    )
    take_gates = pltpu.make_async_remote_copy(
        src_ref=gates.at[:, peer_rows], dst_ref=gates.at[:, peer_rows],
        send_sem=gate_s, recv_sem=gate_r, **peer,
    )
    send_gates.start()
    send_rows.start()

    def answer(k, carry):
        pl.semaphore_signal(ready, inc=1, **sp(k))
        return carry

    lax.fori_loop(0, me, answer, 0)

    pieces = 2
    piece_rows = own // pieces
    spans = [slice(i * piece_rows, (i + 1) * piece_rows) for i in range(pieces)]

    def project(p, rows, dst):
        for at in spans:
            dst[p][at, :] = jnp.dot(
                rows[at, :], w_all[p][...], preferred_element_type=F32
            ).astype(BF16)

    def head_gains():
        gains = hg[...].astype(F32)
        gains = jnp.where(side == 0, gains[0:heads], gains[heads : 2 * heads])
        return jnp.concatenate([gains[i : i + 1] for i in range(heads)], axis=1)

    def sig_piece(rows, dst, i):
        at = spans[i]
        value = jnp.dot(rows[at, :], w_all[OG_][...], preferred_element_type=F32).astype(BF16)
        dst[at, :] = head_gains() * jax.nn.sigmoid(value.astype(F32))

    def piece_of(p, rows, dst, i):
        at = spans[i]
        dst[p][at, :] = jnp.dot(
            rows[at, :], w_all[p][...], preferred_element_type=F32
        ).astype(BF16)

    lane_tiles = range(local_width // 128)

    def prod_piece(rows, proj, prod, i):
        at = spans[i]
        value = jnp.dot(rows[at, :], w_all[CI_][...], preferred_element_type=F32).astype(BF16)
        product = (proj[GI_][at, :].astype(F32) * value.astype(F32)).astype(BF16).astype(F32)
        for c in lane_tiles:
            prod[c, 8 + i * piece_rows : 8 + (i + 1) * piece_rows, :] = product[
                :, c * 128 : (c + 1) * 128
            ]

    w_copies[K_].wait()
    w_copies[V_].wait()
    for copy in w_copies[2:4] + [head_copy] + w_copies[4:]:
        copy.start()
    for copy in [taps_copy, init_copy] + out_copies:
        copy.start()
    project(K_, x_own, proj_own)
    project(V_, x_own, proj_own)
    w_copies[Q_].wait()
    w_copies[OG_].wait()
    head_copy.wait()
    for copy in gate_copies:
        copy.wait()
    take_gates.wait_recv()

    lanes = lax.broadcasted_iota(jnp.int32, (nblocks * heads, BLOCK), 1)
    head_rows = lax.broadcasted_iota(jnp.int32, (heads, BLOCK), 0)
    bias_in = jnp.zeros((heads, BLOCK), F32)
    bias_forget = jnp.zeros((heads, BLOCK), F32)
    for h in range(heads):
        for part_index in range(2):
            pick = (head_rows == h) & (side == part_index)
            c = part_index * heads + h
            bias_in = jnp.where(pick, ib[0:1, c : c + 1], bias_in)
            bias_forget = jnp.where(pick, fb[0:1, c : c + 1], bias_forget)
    ins, forgets = [], []
    for b in range(nblocks):
        at = slice(b * BLOCK, (b + 1) * BLOCK)
        pre = gates[:, at]
        ins.append(jnp.where(side == 0, pre[0:heads], pre[heads : 2 * heads]) + bias_in)
        forget = (
            jnp.where(side == 0, pre[2 * heads : 3 * heads], pre[3 * heads : 4 * heads])
            + bias_forget
        )
        forgets.append(
            jnp.minimum(forget, 0.0) - jnp.log1p(jnp.exp(-jnp.abs(forget))) + fe[:, at]
        )
    ins = jnp.concatenate(ins, axis=0)
    cumulative = jnp.concatenate(forgets, axis=0)
    shift = 1
    while shift < BLOCK:
        cumulative = cumulative + jnp.where(
            lanes >= shift, pltpu.roll(cumulative, shift, 1), 0.0
        )
        shift *= 2
    pair = ins - cumulative
    top = pair
    shift = 1
    while shift < BLOCK:
        top = jnp.maximum(top, jnp.where(lanes >= shift, pltpu.roll(top, shift, 1), top))
        shift *= 2
    total = jnp.broadcast_to(cumulative[:, BLOCK - 1 :], cumulative.shape)
    last_top = jnp.broadcast_to(top[:, BLOCK - 1 :], top.shape)
    log_scale = jnp.full((heads, BLOCK), LOWEST_LOG, F32)
    before = jnp.zeros((heads, BLOCK), F32)
    scales, befores, alphas, betas = [], [], [], []
    for b in range(nblocks):
        block_total = total[b * heads : (b + 1) * heads]
        block_top = block_total + last_top[b * heads : (b + 1) * heads]
        scales.append(log_scale)
        befores.append(before)
        merged = jnp.maximum(block_total + log_scale, block_top)
        alphas.append(block_total + log_scale - merged)
        betas.append(block_top - merged)
        log_scale = merged
        before = before + block_total
    scal[0:heads, :] = before
    scal[heads : 2 * heads, :] = log_scale
    scal_in[me] = scal[...]
    scales = jnp.concatenate(scales, axis=0)
    row_top = jnp.maximum(scales, top)
    table[T_BIAS] = pair + key_log
    table[T_KW] = jnp.exp(pair + key_log - last_top)
    table[T_ALPHA] = jnp.exp(jnp.concatenate(alphas, axis=0))
    table[T_BETA] = jnp.exp(jnp.concatenate(betas, axis=0))
    table[T_TOP] = row_top
    table[T_CARRY] = jnp.concatenate(befores, axis=0)
    carry_weight = jnp.exp(scales - row_top)
    fill = jnp.zeros((BLOCK - 2 * heads, BLOCK), F32)
    for b in range(nblocks):
        rows = slice(b * heads, (b + 1) * heads)
        cols[b] = jnp.concatenate([row_top[rows], carry_weight[rows], fill], axis=0).T
    project(Q_, x_own, proj_own)
    sig_piece(x_own, sig_own, 0)
    sig_piece(x_own, sig_own, 1)

    def weigh_keys(proj, first):
        weighted = []
        for i in range(half_blocks):
            rows = slice(i * BLOCK, (i + 1) * BLOCK)
            b = first + i
            for h in range(heads):
                turned = proj[K_][rows, h * dh : (h + 1) * dh].T
                keys[b, h, :, 0:BLOCK] = turned
                weighted.append(
                    (turned.astype(F32) * table[T_KW, pl.ds(b * heads + h, 1), :]).astype(BF16)
                )
        return weighted

    def block_terms(weighted, proj, first):
        for i in range(half_blocks):
            rows = slice(i * BLOCK, (i + 1) * BLOCK)
            for h in range(heads):
                terms[first + i, h] = jnp.dot(
                    weighted[i * heads + h], proj[V_][rows, h * dh : (h + 1) * dh],
                    preferred_element_type=F32,
                )

    w_copies[GI_].wait()
    w_copies[CI_].wait()
    w_copies[GO_].wait()
    take_rows = pltpu.make_async_remote_copy(
        src_ref=x_own, dst_ref=x_peer, send_sem=tok_s, recv_sem=tok_r, **peer
    )
    take_rows.wait_recv()
    out_weights = [
        pltpu.make_async_remote_copy(
            src_ref=src, dst_ref=dst, send_sem=ow_s.at[i], recv_sem=ow_r.at[i], **peer
        )
        for i, (src, dst) in enumerate(((out_conv, woc_in), (out_memory, wom_in)))
    ]
    for copy in out_weights:
        copy.start()
    weighted_own = weigh_keys(proj_own, my_block)
    project(K_, x_peer, proj_peer)
    block_terms(weighted_own, proj_own, my_block)
    weighted_peer = weigh_keys(proj_peer, peer_block)
    project(V_, x_peer, proj_peer)
    block_terms(weighted_peer, proj_peer, peer_block)

    @pl.when(me < n_sp - 1)
    def _():
        pl.semaphore_wait(ready, n_sp - 1 - me)

    piece_of(GI_, x_own, proj_own, 0)
    for h in range(heads):
        held = jnp.zeros((dh, dh), F32)
        for b in range(nblocks):
            at = pl.ds(b * heads + h, 1)
            keys[b, h, :, BLOCK:] = held.astype(BF16)
            held = table[T_ALPHA, at, :] * held + table[T_BETA, at, :] * terms[b, h]
        for piece in range(per_head):
            seg[h * per_head + piece] = held[
                piece * slice_rows : (piece + 1) * slice_rows, :
            ].astype(BF16)
    seg_in[me] = seg[me]

    def segment_copies(target):
        return (
            pltpu.make_async_remote_copy(
                src_ref=scal, dst_ref=scal_in.at[me],
                send_sem=scal_s, recv_sem=scal_r, **sp(target),
            ),
            pltpu.make_async_remote_copy(
                src_ref=seg.at[target], dst_ref=seg_in.at[me],
                send_sem=seg_s, recv_sem=seg_r, **sp(target),
            ),
        )

    def all_copies(dst, send, recv):
        slots = dst.at[pl.ds(0, n_sp - 1)]
        return pltpu.make_async_remote_copy(
            src_ref=slots, dst_ref=slots, send_sem=send, recv_sem=recv,
            **sp(lax.rem(me + 1, n_sp)),
        )

    all_scales = all_copies(scal_in, scal_s, scal_r)
    all_segments = all_copies(seg_in, seg_s, seg_r)
    all_states = all_copies(state_in, st_s, st_r)

    for k in range(1, n_sp):
        for copy in segment_copies(lax.rem(me + k, n_sp)):
            copy.start()
    piece_of(GI_, x_own, proj_own, 1)

    t_index = lax.broadcasted_iota(jnp.int32, (BLOCK, BLOCK), 0)
    s_index = lax.broadcasted_iota(jnp.int32, (BLOCK, BLOCK), 1)
    causal = s_index <= t_index

    def read_blocks(proj, read, first, chunks, middle=None):
        def scores_of(i):
            rows = slice(i * BLOCK, (i + 1) * BLOCK)
            return [
                jnp.dot(
                    proj[Q_][rows, h * dh : (h + 1) * dh], keys[first + i, h],
                    preferred_element_type=F32,
                )
                for h in range(heads)
            ]

        def weigh(i, raw):
            columns = cols[first + i]
            weighted, carried = [], []
            for h in range(heads):
                log_weight = jnp.where(
                    causal,
                    table[T_BIAS, pl.ds((first + i) * heads + h, 1), :] - columns[:, h : h + 1],
                    -jnp.inf,
                )
                weighted.append((jnp.exp(log_weight) * raw[h][:, 0:BLOCK]).astype(BF16))
                carried.append(columns[:, heads + h : heads + h + 1] * raw[h][:, BLOCK:])
            return weighted, carried

        def read_out(i, weighted, carried):
            rows = slice(i * BLOCK, (i + 1) * BLOCK)
            for h in range(heads):
                hs = slice(h * dh, (h + 1) * dh)
                read[rows, hs] = carried[h] + jnp.dot(
                    weighted[h], proj[V_][rows, hs], preferred_element_type=F32
                )

        raw = scores_of(0)
        for i in range(half_blocks):
            parts = weigh(i, raw)
            chunks[i]()
            if i + 1 < half_blocks:
                raw = scores_of(i + 1)
            read_out(i, *parts)
            if middle is not None and i + 1 == half_blocks // 2:
                middle()
        for chunk in chunks[half_blocks:]:
            chunk()

    read_blocks(
        proj_own, read_own, my_block,
        [
            lambda: prod_piece(x_own, proj_own, prod_own, 0),
            lambda: prod_piece(x_own, proj_own, prod_own, 1),
            lambda: piece_of(GI_, x_peer, proj_peer, 0),
            lambda: piece_of(GI_, x_peer, proj_peer, 1),
        ],
    )
    prod_piece(x_peer, proj_peer, prod_peer, 0)
    prod_piece(x_peer, proj_peer, prod_peer, 1)

    def rim_copy(target):
        return pltpu.make_async_remote_copy(
            src_ref=rim_out, dst_ref=rim_in,
            send_sem=rim_s, recv_sem=rim_r, **sp(target),
        )

    last = me == n_sp - 1
    rim_out[...] = jnp.where(side == 0, prod_peer[:, own : own + 8, :], prod_own[:, own : own + 8, :])

    @pl.when(jnp.logical_not(last))
    def _():
        rim_copy(me + 1).start()

    def owner_step():
        init_copy.wait()

        all_scales.wait_recv()
        all_segments.wait_recv()
        state = init[...]
        state_log = jnp.zeros((1, BLOCK), F32)
        for i in range(n_sp):
            state_out[i] = state.astype(BF16)
            if i == n_sp - 1:
                break
            span = scal_in[i, pl.ds(my_head, 1), :]
            span_top = scal_in[i, pl.ds(heads + my_head, 1), :]
            merged = jnp.maximum(span + state_log, span_top)
            state = (
                jnp.exp(span + state_log - merged) * state
                + jnp.exp(span_top - merged) * seg_in[i].astype(F32)
            )
            state_log = merged
        state_in[me] = state_out[me]

        for k in range(1, n_sp):
            target = lax.rem(me + k, n_sp)
            pltpu.make_async_remote_copy(
                src_ref=state_out.at[target], dst_ref=state_in.at[me],
                send_sem=st_s, recv_sem=st_r, **sp(target),
            ).start()

    along_x, along_z = lax.rem(me, 4), me // 4
    lateness = 2 * along_z + jnp.where(along_x == 3, 3, 2 * along_x)
    late = lateness >= 7
    between = (lateness >= 4) & (lateness < 7)
    soon = (lateness >= 1) & (lateness < 4)
    first = lateness < 1
    pl.when(late)(owner_step)

    project(Q_, x_peer, proj_peer)

    pl.when(between)(owner_step)

    read_blocks(
        proj_peer, read_peer, peer_block,
        [
            lambda: piece_of(GO_, x_peer, proj_peer, 0),
            lambda: piece_of(GO_, x_peer, proj_peer, 1),
            lambda: piece_of(GO_, x_own, proj_own, 0),
            lambda: piece_of(GO_, x_own, proj_own, 1),
        ],
        middle=lambda: pl.when(soon)(owner_step),
    )

    pl.when(first)(owner_step)

    taps_copy.wait()
    for copy in out_copies:
        copy.wait()
    tap_rows = taps[:, pl.ds(my_lane, local_width)].astype(F32)
    conv_rows = 64

    def convolve(proj, prod, dst, part):
        for i in part:
            rows = slice(i * conv_rows, (i + 1) * conv_rows)
            for c in lane_tiles:
                lanes_at = slice(c * 128, (c + 1) * 128)
                mixed = prod[c, i * conv_rows + 6 : i * conv_rows + 6 + conv_rows, :] * tap_rows[
                    0:1, lanes_at
                ]
                for j in range(1, 3):
                    start = i * conv_rows + 6 + j
                    mixed = mixed + prod[c, start : start + conv_rows, :] * tap_rows[
                        j : j + 1, lanes_at
                    ]
                dst[rows, lanes_at] = (proj[GO_][rows, lanes_at].astype(F32) * mixed).astype(BF16)

    conv_steps = range(own // conv_rows)
    send_conv = pltpu.make_async_remote_copy(
        src_ref=conv_peer, dst_ref=conv_in, send_sem=conv_s, recv_sem=conv_r, **peer
    )

    @pl.when(me == 0)
    def _():
        rim_in[...] = jnp.zeros_like(rim_in)

    @pl.when(me > 0)
    def _():
        rim_copy(me - 1).wait_recv()

    prod_own[:, 0:8, :] = jnp.where(side == 0, rim_in[...], prod_peer[:, own : own + 8, :])
    prod_peer[:, 0:8, :] = jnp.where(side == 0, prod_own[:, own : own + 8, :], rim_in[...])
    start_log = jnp.zeros((heads, BLOCK), F32)
    for i in range(n_sp - 1):
        merged = jnp.maximum(scal_in[i, 0:heads, :] + start_log, scal_in[i, heads : 2 * heads, :])
        start_log = jnp.where(i < me, merged, start_log)
    carried_log = table[T_CARRY] + jnp.concatenate([start_log] * nblocks, axis=0)
    new_top = jnp.maximum(table[T_TOP], carried_log)
    keep = jnp.exp(table[T_TOP] - new_top)
    bring = jnp.exp(carried_log - new_top)
    for b in range(nblocks):
        rows = slice(b * heads, (b + 1) * heads)
        cols_in[b] = jnp.concatenate([keep[rows], bring[rows], fill], axis=0).T

    def scale_parts(proj, read, first):
        for block in range(half_blocks):
            rows = slice(block * BLOCK, (block + 1) * BLOCK)
            columns = cols_in[first + block]
            for h in range(heads):
                hs = slice(h * dh, (h + 1) * dh)
                read[rows, hs] = columns[:, h : h + 1] * read[rows, hs]
                proj[Q_][rows, hs] = (
                    columns[:, heads + h : heads + h + 1] * proj[Q_][rows, hs].astype(F32)
                ).astype(BF16)

    half_steps = len(conv_steps) // 2
    convolve(proj_peer, prod_peer, conv_peer, conv_steps[:half_steps])
    sig_piece(x_peer, sig_peer, 0)
    convolve(proj_peer, prod_peer, conv_peer, conv_steps[half_steps:])
    send_conv.start()
    scale_parts(proj_peer, read_peer, peer_block)
    sig_piece(x_peer, sig_peer, 1)
    convolve(proj_own, prod_own, conv_own, conv_steps[:half_steps])
    acc[spans[0], :] = jnp.dot(conv_own[spans[0], :], woc[...], preferred_element_type=F32)
    convolve(proj_own, prod_own, conv_own, conv_steps[half_steps:])
    scale_parts(proj_own, read_own, my_block)
    acc[spans[1], :] = jnp.dot(conv_own[spans[1], :], woc[...], preferred_element_type=F32)
    column = acc.shape[1] // 4

    all_states.wait_recv()
    send_conv.wait_recv()
    for copy in out_weights:
        copy.wait_recv()

    piece_blocks = piece_rows // BLOCK

    def bring_in(proj, piece):
        return [
            [
                jnp.dot(
                    proj[Q_][block * BLOCK : (block + 1) * BLOCK, h * dh : (h + 1) * dh],
                    state_in[h * per_head : (h + 1) * per_head].reshape(dh, dh),
                    preferred_element_type=F32,
                )
                for h in range(heads)
            ]
            for block in range(piece * piece_blocks, (piece + 1) * piece_blocks)
        ]

    def finish(brought, read, sig, dst, piece):
        for i in range(piece_blocks):
            block = piece * piece_blocks + i
            rows = slice(block * BLOCK, (block + 1) * BLOCK)
            for h in range(heads):
                hs = slice(h * dh, (h + 1) * dh)
                readout = read[rows, hs] + brought[i][h]
                normalized = readout * lax.rsqrt(
                    jnp.mean(readout * readout, axis=-1, keepdims=True) + EPSILON
                )
                dst[i * BLOCK : (i + 1) * BLOCK, hs] = (normalized * sig[rows, hs]).astype(BF16)

    def send_memory(i, mem):
        return pltpu.make_async_remote_copy(
            src_ref=mem, dst_ref=mem_in.at[i], send_sem=mem_s.at[i], recv_sem=mem_r.at[i], **peer
        )

    def conv_part(j):
        at = slice(j * column, (j + 1) * column)
        acc[:, at] = acc[:, at] + jnp.dot(
            conv_in[...], woc_in[:, at], preferred_element_type=F32
        )

    def own_part(i, mem):
        acc[spans[i], :] = acc[spans[i], :] + jnp.dot(
            mem[...], wom[...], preferred_element_type=F32
        )

    brought_0 = bring_in(proj_peer, 0)
    conv_part(0)
    brought_1 = bring_in(proj_peer, 1)
    finish(brought_0, read_peer, sig_peer, mem_0, 0)
    send_memory(0, mem_0).start()
    conv_part(1)
    brought_2 = bring_in(proj_own, 0)
    finish(brought_1, read_peer, sig_peer, mem_1, 1)
    send_memory(1, mem_1).start()
    conv_part(2)
    brought_3 = bring_in(proj_own, 1)
    finish(brought_2, read_own, sig_own, mem_2, 0)
    conv_part(3)
    finish(brought_3, read_own, sig_own, mem_3, 1)
    own_part(0, mem_2)
    own_part(1, mem_3)

    for i in range(pieces):
        send_memory(i, (mem_0, mem_1)[i]).wait_recv()

    send_rows.wait_send()
    send_gates.wait_send()

    @pl.when(jnp.logical_not(last))
    def _():
        rim_copy(me + 1).wait_send()

    all_scales.wait_send()
    all_segments.wait_send()
    all_states.wait_send()
    send_conv.wait_send()
    for copy in out_weights:
        copy.wait_send()
    for i, mem in enumerate((mem_0, mem_1)):
        send_memory(i, mem).wait_send()


def last_kernel(acc, mem_in, wom_in, out, stage, sems):
    rows = acc.shape[0] // 4
    copies = []
    for i in range(4):
        at = slice(i * rows, (i + 1) * rows)
        stage[at, :] = (
            acc[at, :]
            + jnp.dot(
                mem_in[i // 2, (i % 2) * rows : (i % 2 + 1) * rows, :], wom_in[...],
                preferred_element_type=F32,
            )
        ).astype(BF16)
        copy = pltpu.make_async_copy(
            stage.at[pl.ds(i * rows, rows), :], out.at[0, pl.ds(i * rows, rows), :], sems.at[i]
        )
        copy.start()
        copies.append(copy)
    for copy in copies:
        copy.wait()


def local_layer(
    n_sp,
    tokens, norm_gain, w_query, w_key, w_value, w_outgate, w_gatein, w_gateout, w_convin,
    w_igate, w_fgate, input_bias, forget_bias, forget_extra, init_memory, head_gain, conv_taps,
    out_memory, out_conv,
):
    own, width = tokens.shape[1:]
    count = 2 * own
    local_width = w_query.shape[1]
    heads, dh = init_memory.shape[1], init_memory.shape[3]
    nblocks = count // BLOCK
    slice_rows = heads * dh // n_sp
    vmem = pltpu.VMEM
    dma = pltpu.SemaphoreType.DMA
    half = vmem((own, local_width), BF16)
    half_wide = vmem((own, local_width), F32)
    quarter = vmem((own // 2, local_width), BF16)
    scratch = [
        vmem((own, width), BF16),
        vmem((width // 128, 128), BF16),
        [vmem((width, local_width), BF16)] * 7,
        vmem((local_width, width), BF16),
        vmem((local_width, width), BF16),
        vmem((2 * heads, width), BF16),
        vmem((2 * heads, width), BF16),
        vmem((4 * heads, count), F32),
        vmem((heads, count), F32),
        vmem((1, 2 * heads), F32),
        vmem((1, 2 * heads), F32),
        vmem(conv_taps.shape, BF16),
        vmem((2 * heads, dh), BF16),
        vmem((slice_rows, dh), F32),
        vmem((own, width), BF16),
        vmem((own, width), BF16),
        [half] * 7,
        [half] * 7,
        half_wide, half_wide,
        half_wide, half_wide,
        half, half, half,
        quarter, quarter, quarter, quarter,
        vmem((local_width, width), BF16),
        vmem((nblocks, heads, dh, 2 * BLOCK), BF16),
        vmem((6, nblocks * heads, BLOCK), F32),
        vmem((nblocks, BLOCK, BLOCK), F32),
        vmem((nblocks, BLOCK, BLOCK), F32),
        vmem((nblocks, heads, dh, dh), F32),
        vmem((n_sp, slice_rows, dh), BF16),
        vmem((n_sp, slice_rows, dh), BF16),
        vmem((2 * heads, BLOCK), F32),
        vmem((n_sp, 2 * heads, BLOCK), F32),
        vmem((n_sp, slice_rows, dh), BF16),
        vmem((n_sp, slice_rows, dh), BF16),
        vmem((local_width // 128, 8, 128), F32),
        vmem((local_width // 128, 8, 128), F32),
        vmem((local_width // 128, own + 8, 128), F32),
        vmem((local_width // 128, own + 8, 128), F32),
        pltpu.SemaphoreType.REGULAR,
        dma((L_W + 7,)),
        dma, dma, dma, dma,
        dma, dma, dma, dma, dma, dma,
        dma, dma,
        dma((2,)), dma((2,)),
        dma, dma,
        dma((2,)), dma((2,)),
    ]
    acc, mem_in, wom_in = pl.pallas_call(
        functools.partial(kernel, n_sp),
        out_shape=(
            vmem((own, width), F32),
            vmem((2, own // 2, local_width), BF16),
            vmem((local_width, width), BF16),
        ),
        in_specs=[pl.BlockSpec(memory_space=pl.ANY)] * 19,
        out_specs=(pl.BlockSpec(memory_space=pltpu.VMEM),) * 3,
        scratch_shapes=scratch,
        compiler_params=pltpu.CompilerParams(
            collective_id=0, has_side_effects=True, vmem_limit_bytes=54 * 1024 * 1024
        ),
    )(
        tokens, norm_gain.reshape(-1, 128),
        w_query, w_key, w_value, w_outgate, w_gatein, w_gateout, w_convin,
        w_igate.T, w_fgate.T, input_bias.reshape(1, -1), forget_bias.reshape(1, -1),
        jnp.swapaxes(forget_extra, 1, 2), init_memory, head_gain.reshape(-1, dh), conv_taps,
        out_memory, out_conv,
    )
    return pl.pallas_call(
        last_kernel,
        out_shape=jax.ShapeDtypeStruct(tokens.shape, BF16),
        in_specs=[pl.BlockSpec(memory_space=pltpu.VMEM)] * 3,
        out_specs=pl.BlockSpec(memory_space=pl.ANY),
        scratch_shapes=[vmem((own, width), BF16), dma((4,))],
        compiler_params=pltpu.CompilerParams(vmem_limit_bytes=16 * 1024 * 1024),
    )(*(pltpu.with_memory_space_constraint(part, pltpu.VMEM) for part in (acc, mem_in, wom_in)))


def solution(mesh):
    rows = P("fs", ("sp", "tp"), None)
    column, replicated = P(None, "tp"), P()
    return jax.shard_map(
        functools.partial(local_layer, mesh.shape["sp"]),
        mesh=mesh,
        in_specs=(
            rows, replicated,
            column, column, column, column, column, column, column,
            replicated, replicated, replicated, replicated,
            P("fs", "sp", "tp"), P("fs", "tp", None, None),
            replicated, replicated,
            P("tp", None), P("tp", None),
        ),
        out_specs=rows,
        check_vma=False,
    )
```

```python
import functools
import math

import jax
import jax.numpy as jnp
from jax import lax
from jax.experimental import pallas as pl
from jax.experimental.pallas import tpu as pltpu
from jax.sharding import PartitionSpec as P

MESH = pl.DeviceIdType.MESH
F32 = jnp.float32
BF16 = jnp.bfloat16
BLOCK = 128
EPSILON = 1e-06
LOWEST_LOG = -1e30

K_, V_, Q_, OG_, GI_, CI_, GO_ = range(7)
T_BIAS, T_KW, T_ALPHA, T_BETA, T_TOP, T_CARRY = range(6)
L_TOK, L_WIG, L_WFG, L_GAIN, L_FE, L_IB, L_FB, L_TAPS, L_HG, L_OM, L_OC, L_INIT, L_W = (
    0, 4, 5, 6, 7, 8, 9, 10, 11, 12, 13, 14, 16,
)


def kernel(
    n_sp,
    tokens, norm_gain, w_query, w_key, w_value, w_outgate, w_gatein, w_gateout, w_convin,
    w_igate, w_fgate, input_bias, forget_bias, forget_extra, init_memory, head_gain, conv_taps,
    out_memory, out_conv,
    acc, mem_in, wom_in,
    tok, gain, w_all, wom, woc, wig, wfg, gates, fe, ib, fb, taps, hg, init, entry,
    x_own, x_peer, proj_own, proj_peer, sig_own, sig_peer, read_own, read_peer,
    conv_own, conv_peer, conv_in, mem_0, mem_1, mem_2, mem_3, woc_in,
    keys, table, cols, cols_in, terms, seg, seg_in, scal, scal_in, state_out, state_in,
    rim_in, rim_out, prod_own, prod_peer,
    ready, lsem, tok_s, tok_r, gate_s, gate_r, seg_s, seg_r, scal_s, scal_r, st_s, st_r,
    rim_s, rim_r, ow_s, ow_r, conv_s, conv_r, mem_s, mem_r,
):
    own = tokens.shape[1]
    count = 2 * own
    local_width = w_query.shape[1]
    heads = init_memory.shape[1]
    dh = init_memory.shape[3]
    nblocks = count // BLOCK
    half_blocks = nblocks // 2
    slice_rows = heads * dh // n_sp
    per_head = dh // slice_rows
    key_log = -0.5 * math.log(dh)
    me = lax.axis_index("sp")
    side = lax.axis_index("tp")
    other = 1 - side
    my_row = pl.multiple_of(side * own, own)
    peer_row = pl.multiple_of(other * own, own)
    my_block = side * half_blocks
    peer_block = other * half_blocks
    my_head = (me * slice_rows) // dh
    my_depth = pl.multiple_of(me * slice_rows - my_head * dh, slice_rows)
    my_lane = pl.multiple_of(side * local_width, local_width)
    my_rows = pl.ds(my_row, own)
    peer_rows = pl.ds(peer_row, own)

    def local(src, dst, index):
        return pltpu.make_async_copy(src, dst, lsem.at[index])

    def sp(target):
        return dict(device_id={"sp": target}, device_id_type=MESH)

    peer = dict(device_id={"tp": other}, device_id_type=MESH)
    weights = (w_key, w_value, w_query, w_outgate, w_gatein, w_convin, w_gateout)

    barrier = pltpu.get_barrier_semaphore()
    chunks = 4
    chunk_rows = own // chunks
    token_copies = [
        local(
            tokens.at[0, pl.ds(c * chunk_rows, chunk_rows), :],
            tok.at[pl.ds(c * chunk_rows, chunk_rows), :],
            L_TOK + c,
        )
        for c in range(chunks)
    ]
    gain_copy = local(norm_gain, gain, L_GAIN)
    narrow_copies = [local(w_igate, wig, L_WIG), local(w_fgate, wfg, L_WFG)]
    w_copies = [local(weights[p], w_all[p], L_W + p) for p in range(7)]
    gate_copies = [
        local(forget_extra.at[0], fe, L_FE),
        local(input_bias, ib, L_IB),
        local(forget_bias, fb, L_FB),
    ]
    head_copy = local(head_gain, hg, L_HG)
    taps_copy = local(conv_taps, taps, L_TAPS)
    init_copy = local(init_memory.at[0], init, L_INIT)
    out_copies = [local(out_conv, woc, L_OC), local(out_memory, wom, L_OM)]
    gain_copy.start()
    for copy in token_copies + narrow_copies + w_copies[:2] + gate_copies:
        copy.start()
    pl.semaphore_signal(barrier, inc=1, **peer)

    def greet(k, carry):
        pl.semaphore_signal(barrier, inc=1, **sp(k))
        return carry

    lax.fori_loop(me + 1, n_sp, greet, 0)

    gain_copy.wait()
    gain_row = jnp.concatenate(
        [gain[i : i + 1, :] for i in range(gain.shape[0])], axis=1
    ).astype(F32)
    norm_rows = 8

    gate_rows = chunk_rows

    def own_gates(c):
        rows = x_own[c * gate_rows : (c + 1) * gate_rows, :]
        gates[:, pl.ds(my_row + c * gate_rows, gate_rows)] = lax.dot_general(
            narrow, rows, (((1,), (1,)), ((), ())), preferred_element_type=F32
        )

    for c in range(chunks):
        token_copies[c].wait()
        if c == 1:
            for copy in narrow_copies:
                copy.wait()
            narrow = jnp.concatenate([wig[...], wfg[...]], axis=0)
        if c > 0:
            own_gates(c - 1)
        for start in range(c * chunk_rows, (c + 1) * chunk_rows, norm_rows):
            rows = slice(start, start + norm_rows)
            values = tok[rows, :].astype(F32)
            scale = lax.rsqrt(jnp.mean(values * values, axis=-1, keepdims=True) + EPSILON)
            x_own[rows, :] = (values * scale * gain_row).astype(BF16)
    own_gates(chunks - 1)

    pl.semaphore_wait(barrier, me + 1)
    send_rows = pltpu.make_async_remote_copy(
        src_ref=x_own, dst_ref=x_peer, send_sem=tok_s, recv_sem=tok_r, **peer
    )
    send_gates = pltpu.make_async_remote_copy(
        src_ref=gates.at[:, my_rows], dst_ref=gates.at[:, my_rows],
        send_sem=gate_s, recv_sem=gate_r, **peer,
    )
    take_gates = pltpu.make_async_remote_copy(
        src_ref=gates.at[:, peer_rows], dst_ref=gates.at[:, peer_rows],
        send_sem=gate_s, recv_sem=gate_r, **peer,
    )
    send_gates.start()
    send_rows.start()

    def answer(k, carry):
        pl.semaphore_signal(ready, inc=1, **sp(k))
        return carry

    lax.fori_loop(0, me, answer, 0)

    pieces = 2
    piece_rows = own // pieces
    spans = [slice(i * piece_rows, (i + 1) * piece_rows) for i in range(pieces)]

    def project(p, rows, dst):
        for at in spans:
            dst[p][at, :] = jnp.dot(
                rows[at, :], w_all[p][...], preferred_element_type=F32
            ).astype(BF16)

    def head_gains():
        gains = hg[...].astype(F32)
        gains = jnp.where(side == 0, gains[0:heads], gains[heads : 2 * heads])
        return jnp.concatenate([gains[i : i + 1] for i in range(heads)], axis=1)

    def sig_piece(rows, dst, i):
        at = spans[i]
        value = jnp.dot(rows[at, :], w_all[OG_][...], preferred_element_type=F32).astype(BF16)
        dst[at, :] = head_gains() * jax.nn.sigmoid(value.astype(F32))

    def piece_of(p, rows, dst, i):
        at = spans[i]
        dst[p][at, :] = jnp.dot(
            rows[at, :], w_all[p][...], preferred_element_type=F32
        ).astype(BF16)

    lane_tiles = range(local_width // 128)

    def prod_piece(rows, proj, prod, i):
        at = spans[i]
        value = jnp.dot(rows[at, :], w_all[CI_][...], preferred_element_type=F32).astype(BF16)
        product = (proj[GI_][at, :].astype(F32) * value.astype(F32)).astype(BF16).astype(F32)
        for c in lane_tiles:
            prod[c, 8 + i * piece_rows : 8 + (i + 1) * piece_rows, :] = product[
                :, c * 128 : (c + 1) * 128
            ]

    w_copies[K_].wait()
    w_copies[V_].wait()
    for copy in w_copies[2:4] + [head_copy] + w_copies[4:]:
        copy.start()
    for copy in [taps_copy, init_copy] + out_copies:
        copy.start()
    project(K_, x_own, proj_own)
    project(V_, x_own, proj_own)
    w_copies[Q_].wait()
    w_copies[OG_].wait()
    head_copy.wait()
    for copy in gate_copies:
        copy.wait()
    take_gates.wait_recv()

    lanes = lax.broadcasted_iota(jnp.int32, (nblocks * heads, BLOCK), 1)
    head_rows = lax.broadcasted_iota(jnp.int32, (heads, BLOCK), 0)
    bias_in = jnp.zeros((heads, BLOCK), F32)
    bias_forget = jnp.zeros((heads, BLOCK), F32)
    for h in range(heads):
        for part_index in range(2):
            pick = (head_rows == h) & (side == part_index)
            c = part_index * heads + h
            bias_in = jnp.where(pick, ib[0:1, c : c + 1], bias_in)
            bias_forget = jnp.where(pick, fb[0:1, c : c + 1], bias_forget)
    ins, forgets = [], []
    for b in range(nblocks):
        at = slice(b * BLOCK, (b + 1) * BLOCK)
        pre = gates[:, at]
        ins.append(jnp.where(side == 0, pre[0:heads], pre[heads : 2 * heads]) + bias_in)
        forget = (
            jnp.where(side == 0, pre[2 * heads : 3 * heads], pre[3 * heads : 4 * heads])
            + bias_forget
        )
        forgets.append(
            jnp.minimum(forget, 0.0) - jnp.log1p(jnp.exp(-jnp.abs(forget))) + fe[:, at]
        )
    ins = jnp.concatenate(ins, axis=0)
    cumulative = jnp.concatenate(forgets, axis=0)
    shift = 1
    while shift < BLOCK:
        cumulative = cumulative + jnp.where(
            lanes >= shift, pltpu.roll(cumulative, shift, 1), 0.0
        )
        shift *= 2
    pair = ins - cumulative
    top = pair
    shift = 1
    while shift < BLOCK:
        top = jnp.maximum(top, jnp.where(lanes >= shift, pltpu.roll(top, shift, 1), top))
        shift *= 2
    total = jnp.broadcast_to(cumulative[:, BLOCK - 1 :], cumulative.shape)
    last_top = jnp.broadcast_to(top[:, BLOCK - 1 :], top.shape)
    log_scale = jnp.full((heads, BLOCK), LOWEST_LOG, F32)
    before = jnp.zeros((heads, BLOCK), F32)
    scales, befores, alphas, betas = [], [], [], []
    for b in range(nblocks):
        block_total = total[b * heads : (b + 1) * heads]
        block_top = block_total + last_top[b * heads : (b + 1) * heads]
        scales.append(log_scale)
        befores.append(before)
        merged = jnp.maximum(block_total + log_scale, block_top)
        alphas.append(block_total + log_scale - merged)
        betas.append(block_top - merged)
        log_scale = merged
        before = before + block_total
    scal[0:heads, :] = before
    scal[heads : 2 * heads, :] = log_scale
    scal_in[me] = scal[...]
    scales = jnp.concatenate(scales, axis=0)
    row_top = jnp.maximum(scales, top)
    table[T_BIAS] = pair + key_log
    table[T_KW] = jnp.exp(pair + key_log - last_top)
    table[T_ALPHA] = jnp.exp(jnp.concatenate(alphas, axis=0))
    table[T_BETA] = jnp.exp(jnp.concatenate(betas, axis=0))
    table[T_TOP] = row_top
    table[T_CARRY] = jnp.concatenate(befores, axis=0)
    carry_weight = jnp.exp(scales - row_top)
    fill = jnp.zeros((BLOCK - 2 * heads, BLOCK), F32)
    for b in range(nblocks):
        rows = slice(b * heads, (b + 1) * heads)
        cols[b] = jnp.concatenate([row_top[rows], carry_weight[rows], fill], axis=0).T
    project(Q_, x_own, proj_own)
    sig_piece(x_own, sig_own, 0)
    sig_piece(x_own, sig_own, 1)

    def weigh_keys(proj, first):
        weighted = []
        for i in range(half_blocks):
            rows = slice(i * BLOCK, (i + 1) * BLOCK)
            b = first + i
            for h in range(heads):
                turned = proj[K_][rows, h * dh : (h + 1) * dh].T
                keys[b, h, :, 0:BLOCK] = turned
                weighted.append(
                    (turned.astype(F32) * table[T_KW, pl.ds(b * heads + h, 1), :]).astype(BF16)
                )
        return weighted

    def block_terms(weighted, proj, first):
        for i in range(half_blocks):
            rows = slice(i * BLOCK, (i + 1) * BLOCK)
            for h in range(heads):
                terms[first + i, h] = jnp.dot(
                    weighted[i * heads + h], proj[V_][rows, h * dh : (h + 1) * dh],
                    preferred_element_type=F32,
                )

    w_copies[GI_].wait()
    w_copies[CI_].wait()
    w_copies[GO_].wait()
    take_rows = pltpu.make_async_remote_copy(
        src_ref=x_own, dst_ref=x_peer, send_sem=tok_s, recv_sem=tok_r, **peer
    )
    take_rows.wait_recv()
    out_weights = [
        pltpu.make_async_remote_copy(
            src_ref=src, dst_ref=dst, send_sem=ow_s.at[i], recv_sem=ow_r.at[i], **peer
        )
        for i, (src, dst) in enumerate(((out_conv, woc_in), (out_memory, wom_in)))
    ]
    for copy in out_weights:
        copy.start()
    weighted_own = weigh_keys(proj_own, my_block)
    project(K_, x_peer, proj_peer)
    block_terms(weighted_own, proj_own, my_block)
    weighted_peer = weigh_keys(proj_peer, peer_block)
    project(V_, x_peer, proj_peer)
    block_terms(weighted_peer, proj_peer, peer_block)

    @pl.when(me < n_sp - 1)
    def _():
        pl.semaphore_wait(ready, n_sp - 1 - me)

    along_x, along_z, size_z = lax.rem(me, 4), me // 4, n_sp // 4
    steps = sorted(
        ((dx, dz) for dx in range(4) for dz in range(size_z) if dx or dz),
        key=lambda step: -min(step[0], 4 - step[0]) - min(step[1], size_z - step[1]),
    )
    targets = [
        lax.rem(along_z + dz, size_z) * 4 + lax.rem(along_x + dx, 4) for dx, dz in steps
    ]
    for target in targets:
        pltpu.make_async_remote_copy(
            src_ref=scal, dst_ref=scal_in.at[me],
            send_sem=scal_s, recv_sem=scal_r, **sp(target),
        ).start()
    piece_of(GI_, x_own, proj_own, 0)
    for h in range(heads):
        held = jnp.zeros((dh, dh), F32)
        for b in range(nblocks):
            at = pl.ds(b * heads + h, 1)
            keys[b, h, :, BLOCK:] = held.astype(BF16)
            held = table[T_ALPHA, at, :] * held + table[T_BETA, at, :] * terms[b, h]
        for piece in range(per_head):
            seg[h * per_head + piece] = held[
                piece * slice_rows : (piece + 1) * slice_rows, :
            ].astype(BF16)
    seg_in[me] = seg[me]

    def all_copies(dst, send, recv):
        slots = dst.at[pl.ds(0, n_sp - 1)]
        return pltpu.make_async_remote_copy(
            src_ref=slots, dst_ref=slots, send_sem=send, recv_sem=recv,
            **sp(lax.rem(me + 1, n_sp)),
        )

    all_scales = all_copies(scal_in, scal_s, scal_r)
    all_segments = all_copies(seg_in, seg_s, seg_r)
    all_states = all_copies(state_in, st_s, st_r)

    for target in targets:
        pltpu.make_async_remote_copy(
            src_ref=seg.at[target], dst_ref=seg_in.at[me],
            send_sem=seg_s, recv_sem=seg_r, **sp(target),
        ).start()
    piece_of(GI_, x_own, proj_own, 1)

    t_index = lax.broadcasted_iota(jnp.int32, (BLOCK, BLOCK), 0)
    s_index = lax.broadcasted_iota(jnp.int32, (BLOCK, BLOCK), 1)
    causal = s_index <= t_index

    def read_blocks(proj, read, first, chunks, middle=None):
        def scores_of(i):
            rows = slice(i * BLOCK, (i + 1) * BLOCK)
            return [
                jnp.dot(
                    proj[Q_][rows, h * dh : (h + 1) * dh], keys[first + i, h],
                    preferred_element_type=F32,
                )
                for h in range(heads)
            ]

        def weigh(i, raw):
            columns = cols[first + i]
            weighted, carried = [], []
            for h in range(heads):
                log_weight = jnp.where(
                    causal,
                    table[T_BIAS, pl.ds((first + i) * heads + h, 1), :] - columns[:, h : h + 1],
                    -jnp.inf,
                )
                weighted.append((jnp.exp(log_weight) * raw[h][:, 0:BLOCK]).astype(BF16))
                carried.append(columns[:, heads + h : heads + h + 1] * raw[h][:, BLOCK:])
            return weighted, carried

        def read_out(i, weighted, carried):
            rows = slice(i * BLOCK, (i + 1) * BLOCK)
            for h in range(heads):
                hs = slice(h * dh, (h + 1) * dh)
                read[rows, hs] = carried[h] + jnp.dot(
                    weighted[h], proj[V_][rows, hs], preferred_element_type=F32
                )

        raw = scores_of(0)
        for i in range(half_blocks):
            parts = weigh(i, raw)
            chunks[i]()
            if i + 1 < half_blocks:
                raw = scores_of(i + 1)
            read_out(i, *parts)
            if middle is not None and i + 1 == half_blocks // 2:
                middle()
        for chunk in chunks[half_blocks:]:
            chunk()

    read_blocks(
        proj_own, read_own, my_block,
        [
            lambda: prod_piece(x_own, proj_own, prod_own, 0),
            lambda: prod_piece(x_own, proj_own, prod_own, 1),
            lambda: piece_of(GI_, x_peer, proj_peer, 0),
            lambda: piece_of(GI_, x_peer, proj_peer, 1),
        ],
    )
    prod_piece(x_peer, proj_peer, prod_peer, 0)
    prod_piece(x_peer, proj_peer, prod_peer, 1)

    def rim_copy(target):
        return pltpu.make_async_remote_copy(
            src_ref=rim_out, dst_ref=rim_in,
            send_sem=rim_s, recv_sem=rim_r, **sp(target),
        )

    last = me == n_sp - 1
    rim_out[...] = jnp.where(side == 0, prod_peer[:, own : own + 8, :], prod_own[:, own : own + 8, :])

    @pl.when(jnp.logical_not(last))
    def _():
        rim_copy(me + 1).start()

    def owner_step():
        init_copy.wait()

        all_scales.wait_recv()
        all_segments.wait_recv()
        state = init[my_head, pl.ds(my_depth, slice_rows), :]
        state_log = jnp.zeros((1, BLOCK), F32)
        for i in range(n_sp):
            state_out[i] = state.astype(BF16)
            if i == n_sp - 1:
                break
            span = scal_in[i, pl.ds(my_head, 1), :]
            span_top = scal_in[i, pl.ds(heads + my_head, 1), :]
            merged = jnp.maximum(span + state_log, span_top)
            state = (
                jnp.exp(span + state_log - merged) * state
                + jnp.exp(span_top - merged) * seg_in[i].astype(F32)
            )
            state_log = merged
        state_in[me] = state_out[me]

        for target in targets:
            pltpu.make_async_remote_copy(
                src_ref=state_out.at[target], dst_ref=state_in.at[me],
                send_sem=st_s, recv_sem=st_r, **sp(target),
            ).start()

    lateness = 2 * along_z + jnp.where(along_x == 1, 2, jnp.where(along_x == 0, 0, 3))
    late = lateness >= 7
    between = (lateness >= 4) & (lateness < 7)
    soon = (lateness >= 1) & (lateness < 4)
    first = lateness < 1
    pl.when(late)(owner_step)

    project(Q_, x_peer, proj_peer)

    pl.when(between)(owner_step)

    read_blocks(
        proj_peer, read_peer, peer_block,
        [
            lambda: piece_of(GO_, x_peer, proj_peer, 0),
            lambda: piece_of(GO_, x_peer, proj_peer, 1),
            lambda: piece_of(GO_, x_own, proj_own, 0),
            lambda: piece_of(GO_, x_own, proj_own, 1),
        ],
        middle=lambda: pl.when(soon)(owner_step),
    )

    pl.when(first)(owner_step)

    taps_copy.wait()
    for copy in out_copies:
        copy.wait()
    tap_rows = taps[:, pl.ds(my_lane, local_width)].astype(F32)
    conv_rows = 64

    def convolve(proj, prod, dst, part):
        for i in part:
            rows = slice(i * conv_rows, (i + 1) * conv_rows)
            for c in lane_tiles:
                lanes_at = slice(c * 128, (c + 1) * 128)
                mixed = prod[c, i * conv_rows + 6 : i * conv_rows + 6 + conv_rows, :] * tap_rows[
                    0:1, lanes_at
                ]
                for j in range(1, 3):
                    start = i * conv_rows + 6 + j
                    mixed = mixed + prod[c, start : start + conv_rows, :] * tap_rows[
                        j : j + 1, lanes_at
                    ]
                dst[rows, lanes_at] = (proj[GO_][rows, lanes_at].astype(F32) * mixed).astype(BF16)

    conv_steps = range(own // conv_rows)
    send_conv = pltpu.make_async_remote_copy(
        src_ref=conv_peer, dst_ref=conv_in, send_sem=conv_s, recv_sem=conv_r, **peer
    )

    @pl.when(me == 0)
    def _():
        rim_in[...] = jnp.zeros_like(rim_in)

    @pl.when(me > 0)
    def _():
        rim_copy(me - 1).wait_recv()

    prod_own[:, 0:8, :] = jnp.where(side == 0, rim_in[...], prod_peer[:, own : own + 8, :])
    prod_peer[:, 0:8, :] = jnp.where(side == 0, prod_own[:, own : own + 8, :], rim_in[...])
    start_log = jnp.zeros((heads, BLOCK), F32)
    for i in range(n_sp - 1):
        merged = jnp.maximum(scal_in[i, 0:heads, :] + start_log, scal_in[i, heads : 2 * heads, :])
        start_log = jnp.where(i < me, merged, start_log)
    carried_log = table[T_CARRY] + jnp.concatenate([start_log] * nblocks, axis=0)
    new_top = jnp.maximum(table[T_TOP], carried_log)
    keep = jnp.exp(table[T_TOP] - new_top)
    bring = jnp.exp(carried_log - new_top)
    for b in range(nblocks):
        rows = slice(b * heads, (b + 1) * heads)
        cols_in[b] = jnp.concatenate([keep[rows], bring[rows], fill], axis=0).T

    def scale_parts(proj, read, first):
        for block in range(half_blocks):
            rows = slice(block * BLOCK, (block + 1) * BLOCK)
            columns = cols_in[first + block]
            for h in range(heads):
                hs = slice(h * dh, (h + 1) * dh)
                read[rows, hs] = columns[:, h : h + 1] * read[rows, hs]
                proj[Q_][rows, hs] = (
                    columns[:, heads + h : heads + h + 1] * proj[Q_][rows, hs].astype(F32)
                ).astype(BF16)

    half_steps = len(conv_steps) // 2
    convolve(proj_peer, prod_peer, conv_peer, conv_steps[:half_steps])
    sig_piece(x_peer, sig_peer, 0)
    convolve(proj_peer, prod_peer, conv_peer, conv_steps[half_steps:])
    send_conv.start()
    scale_parts(proj_peer, read_peer, peer_block)
    sig_piece(x_peer, sig_peer, 1)
    convolve(proj_own, prod_own, conv_own, conv_steps[:half_steps])
    acc[spans[0], :] = jnp.dot(conv_own[spans[0], :], woc[...], preferred_element_type=F32)
    convolve(proj_own, prod_own, conv_own, conv_steps[half_steps:])
    scale_parts(proj_own, read_own, my_block)
    acc[spans[1], :] = jnp.dot(conv_own[spans[1], :], woc[...], preferred_element_type=F32)
    column = acc.shape[1] // 4

    @pl.when(me == 0)
    def _():
        entry[...] = init[...].reshape(entry.shape).astype(BF16)

    @pl.when(me > 0)
    def _():
        all_states.wait_recv()
        entry[...] = state_in[...]

    send_conv.wait_recv()
    for copy in out_weights:
        copy.wait_recv()

    piece_blocks = piece_rows // BLOCK

    def bring_in(proj, piece):
        return [
            [
                jnp.dot(
                    proj[Q_][block * BLOCK : (block + 1) * BLOCK, h * dh : (h + 1) * dh],
                    entry[h * per_head : (h + 1) * per_head].reshape(dh, dh),
                    preferred_element_type=F32,
                )
                for h in range(heads)
            ]
            for block in range(piece * piece_blocks, (piece + 1) * piece_blocks)
        ]

    def finish(brought, read, sig, dst, piece):
        for i in range(piece_blocks):
            block = piece * piece_blocks + i
            rows = slice(block * BLOCK, (block + 1) * BLOCK)
            for h in range(heads):
                hs = slice(h * dh, (h + 1) * dh)
                readout = read[rows, hs] + brought[i][h]
                normalized = readout * lax.rsqrt(
                    jnp.mean(readout * readout, axis=-1, keepdims=True) + EPSILON
                )
                dst[i * BLOCK : (i + 1) * BLOCK, hs] = (normalized * sig[rows, hs]).astype(BF16)

    def send_memory(i, mem):
        return pltpu.make_async_remote_copy(
            src_ref=mem, dst_ref=mem_in.at[i], send_sem=mem_s.at[i], recv_sem=mem_r.at[i], **peer
        )

    def conv_part(j):
        at = slice(j * column, (j + 1) * column)
        acc[:, at] = acc[:, at] + jnp.dot(
            conv_in[...], woc_in[:, at], preferred_element_type=F32
        )

    def own_part(i, mem):
        acc[spans[i], :] = acc[spans[i], :] + jnp.dot(
            mem[...], wom[...], preferred_element_type=F32
        )

    brought_0 = bring_in(proj_peer, 0)
    conv_part(0)
    brought_1 = bring_in(proj_peer, 1)
    finish(brought_0, read_peer, sig_peer, mem_0, 0)
    send_memory(0, mem_0).start()
    conv_part(1)
    brought_2 = bring_in(proj_own, 0)
    finish(brought_1, read_peer, sig_peer, mem_1, 1)
    send_memory(1, mem_1).start()
    conv_part(2)
    brought_3 = bring_in(proj_own, 1)
    finish(brought_2, read_own, sig_own, mem_2, 0)
    conv_part(3)
    finish(brought_3, read_own, sig_own, mem_3, 1)
    own_part(0, mem_2)
    own_part(1, mem_3)

    for i in range(pieces):
        send_memory(i, (mem_0, mem_1)[i]).wait_recv()

    send_rows.wait_send()
    send_gates.wait_send()

    @pl.when(jnp.logical_not(last))
    def _():
        rim_copy(me + 1).wait_send()

    @pl.when(me == 0)
    def _():
        all_states.wait_recv()

    all_scales.wait_send()
    all_segments.wait_send()
    all_states.wait_send()
    send_conv.wait_send()
    for copy in out_weights:
        copy.wait_send()
    for i, mem in enumerate((mem_0, mem_1)):
        send_memory(i, mem).wait_send()


def last_kernel(acc, mem_in, wom_in, out, stage, sems):
    rows = acc.shape[0] // 4
    copies = []
    for i in range(4):
        at = slice(i * rows, (i + 1) * rows)
        stage[at, :] = (
            acc[at, :]
            + jnp.dot(
                mem_in[i // 2, (i % 2) * rows : (i % 2 + 1) * rows, :], wom_in[...],
                preferred_element_type=F32,
            )
        ).astype(BF16)
        copy = pltpu.make_async_copy(
            stage.at[pl.ds(i * rows, rows), :], out.at[0, pl.ds(i * rows, rows), :], sems.at[i]
        )
        copy.start()
        copies.append(copy)
    for copy in copies:
        copy.wait()


def local_layer(
    n_sp,
    tokens, norm_gain, w_query, w_key, w_value, w_outgate, w_gatein, w_gateout, w_convin,
    w_igate, w_fgate, input_bias, forget_bias, forget_extra, init_memory, head_gain, conv_taps,
    out_memory, out_conv,
):
    own, width = tokens.shape[1:]
    count = 2 * own
    local_width = w_query.shape[1]
    heads, dh = init_memory.shape[1], init_memory.shape[3]
    nblocks = count // BLOCK
    slice_rows = heads * dh // n_sp
    vmem = pltpu.VMEM
    dma = pltpu.SemaphoreType.DMA
    half = vmem((own, local_width), BF16)
    half_wide = vmem((own, local_width), F32)
    quarter = vmem((own // 2, local_width), BF16)
    scratch = [
        vmem((own, width), BF16),
        vmem((width // 128, 128), BF16),
        [vmem((width, local_width), BF16)] * 7,
        vmem((local_width, width), BF16),
        vmem((local_width, width), BF16),
        vmem((2 * heads, width), BF16),
        vmem((2 * heads, width), BF16),
        vmem((4 * heads, count), F32),
        vmem((heads, count), F32),
        vmem((1, 2 * heads), F32),
        vmem((1, 2 * heads), F32),
        vmem(conv_taps.shape, BF16),
        vmem((2 * heads, dh), BF16),
        vmem((heads, dh, dh), F32),
        vmem((n_sp, slice_rows, dh), BF16),
        vmem((own, width), BF16),
        vmem((own, width), BF16),
        [half] * 7,
        [half] * 7,
        half_wide, half_wide,
        half_wide, half_wide,
        half, half, half,
        quarter, quarter, quarter, quarter,
        vmem((local_width, width), BF16),
        vmem((nblocks, heads, dh, 2 * BLOCK), BF16),
        vmem((6, nblocks * heads, BLOCK), F32),
        vmem((nblocks, BLOCK, BLOCK), F32),
        vmem((nblocks, BLOCK, BLOCK), F32),
        vmem((nblocks, heads, dh, dh), F32),
        vmem((n_sp, slice_rows, dh), BF16),
        vmem((n_sp, slice_rows, dh), BF16),
        vmem((2 * heads, BLOCK), F32),
        vmem((n_sp, 2 * heads, BLOCK), F32),
        vmem((n_sp, slice_rows, dh), BF16),
        vmem((n_sp, slice_rows, dh), BF16),
        vmem((local_width // 128, 8, 128), F32),
        vmem((local_width // 128, 8, 128), F32),
        vmem((local_width // 128, own + 8, 128), F32),
        vmem((local_width // 128, own + 8, 128), F32),
        pltpu.SemaphoreType.REGULAR,
        dma((L_W + 7,)),
        dma, dma, dma, dma,
        dma, dma, dma, dma, dma, dma,
        dma, dma,
        dma((2,)), dma((2,)),
        dma, dma,
        dma((2,)), dma((2,)),
    ]
    acc, mem_in, wom_in = pl.pallas_call(
        functools.partial(kernel, n_sp),
        out_shape=(
            vmem((own, width), F32),
            vmem((2, own // 2, local_width), BF16),
            vmem((local_width, width), BF16),
        ),
        in_specs=[pl.BlockSpec(memory_space=pl.ANY)] * 19,
        out_specs=(pl.BlockSpec(memory_space=pltpu.VMEM),) * 3,
        scratch_shapes=scratch,
        compiler_params=pltpu.CompilerParams(
            collective_id=0, has_side_effects=True, vmem_limit_bytes=54 * 1024 * 1024
        ),
    )(
        tokens, norm_gain.reshape(-1, 128),
        w_query, w_key, w_value, w_outgate, w_gatein, w_gateout, w_convin,
        w_igate.T, w_fgate.T, input_bias.reshape(1, -1), forget_bias.reshape(1, -1),
        jnp.swapaxes(forget_extra, 1, 2), init_memory, head_gain.reshape(-1, dh), conv_taps,
        out_memory, out_conv,
    )
    return pl.pallas_call(
        last_kernel,
        out_shape=jax.ShapeDtypeStruct(tokens.shape, BF16),
        in_specs=[pl.BlockSpec(memory_space=pltpu.VMEM)] * 3,
        out_specs=pl.BlockSpec(memory_space=pl.ANY),
        scratch_shapes=[vmem((own, width), BF16), dma((4,))],
        compiler_params=pltpu.CompilerParams(vmem_limit_bytes=16 * 1024 * 1024),
    )(*(pltpu.with_memory_space_constraint(part, pltpu.VMEM) for part in (acc, mem_in, wom_in)))


def solution(mesh):
    rows = P("fs", ("sp", "tp"), None)
    column, replicated = P(None, "tp"), P()
    return jax.shard_map(
        functools.partial(local_layer, mesh.shape["sp"]),
        mesh=mesh,
        in_specs=(
            rows, replicated,
            column, column, column, column, column, column, column,
            replicated, replicated, replicated, replicated,
            P("fs", "sp", "tp"), P("fs", "tp", None, None),
            replicated, replicated,
            P("tp", None), P("tp", None),
        ),
        out_specs=rows,
        check_vma=False,
    )
```
